128 devices in a mesh: sp: 32 (over z, y, core), tp: 4 (over x).
Axes of the slice: x: 4, y: 4, z: 4, core: 2. Of those that a mesh axis runs over, the one named last changes fastest.
Arguments:
- output_cotangent: bfloat16 [12288, 2048], P('sp'), may hold values from -8 to 8
- chosen_expert_index: int32 [12288, 2], P('sp'), may hold values from 0 to 31, all different within a row; in each aligned block of 384 rows (0 to 383, 384 to 767, ...) at most 40 rows name the same one
- chosen_expert_weight: float32 [12288, 2], P('sp'), may hold values from 0.2 to 1
- expert_slot_tokens: bfloat16 [32, 1280, 2048], P('sp'), may hold values from -48 to 48, as said below
- expert_gate_matrix: bfloat16 [32, 2048, 2048], P('sp', None, 'tp'), may hold values from -0.125 to 0.125
- expert_up_matrix: bfloat16 [32, 2048, 2048], P('sp', None, 'tp'), may hold values from -0.125 to 0.125
- expert_down_matrix: bfloat16 [32, 2048, 2048], P('sp', 'tp'), may hold values from -0.125 to 0.125
- output_projection_matrix: bfloat16 [2048, 2048], P(None, 'tp'), may hold values from -0.125 to 0.125
- recurrence_input: bfloat16 [12288, 2048], P('sp', 'tp'), may hold values from -6 to 6
- branch_activation_values: bfloat16 [12288, 2048], P('sp', 'tp'), may hold values from -6 to 6
- forward_scan_state: float32 [12288, 2048], P('sp', 'tp'), may hold values from -6 to 6
- reverse_scan_state: float32 [12288, 2048], P('sp', 'tp'), may hold values from -6 to 6
- channel_decay_rate: float32 [2048], P('tp'), may hold values from 5.08626302e-07 to 0.01
- position_extra_log_decay: float32 [12288], P('sp'), may hold values from -0.7 to 0, as said below
- recurrence_gate_weights: bfloat16 [8, 256, 256], P('tp'), may hold values from -0.375 to 0.375
- input_gate_weights: bfloat16 [8, 256, 256], P('tp'), may hold values from -0.375 to 0.375
Outputs:
- expert_gate_grad: bfloat16 [32, 2048, 2048], P('sp', None, 'tp')
- expert_up_grad: bfloat16 [32, 2048, 2048], P('sp', None, 'tp')
- expert_down_grad: bfloat16 [32, 2048, 2048], P('sp', 'tp')
- proj_grad: float32 [2048, 2048], P('sp', 'tp')
- branch_grad: bfloat16 [12288, 2048], P('sp', 'tp')
- input_grad: bfloat16 [12288, 2048], P('sp', 'tp')
The draws below stay inside these ranges and needn't reach their ends.
Inputs may be any that keep to these rules, and one draw needn't show every extreme that they name: `chosen_expert_index`: each row names 2 different experts; among the rows of one index of sp no expert is named more than 40 times, a bound that some block reaches. `expert_slot_tokens`: row s * 40 + c of expert e holds the input of slot c that source s fills for e, slots filled as the steps number them. `position_extra_log_decay`: zero except at a few positions.
All inputs are finite; a program needn't handle non-finite values.
Results may differ from the reference program's by a relative error of at most 0.022.
Values may be sent and summed in bfloat16 or wider, within the bound.
No kernel may reach another device: no remote copies, remote signals or barrier semaphores. Data moves between devices by JAX's collectives and lax.ppermute only.
A program may use at most 192 MiB of HBM per device.

```python
import math
import jax
import jax.numpy as jnp
import numpy as np
from jax import lax

D = 2048
DR = 2048
BLOCKS = 8
BW = 256
FF = 2048
EXPERTS = 32
TOP = 2
TOK_DEV = 384
TOKENS = 12288
CAP = 40
RECV = 1280
N_SP = 32
N_TP = 4


def draw_expert_slot_tokens(key, part):
    scale_key = jax.random.fold_in(key, 11)
    value_key = jax.random.fold_in(key, 12)
    scales = jnp.exp(jax.random.uniform(scale_key, (EXPERTS, RECV, 1), jnp.float32, math.log(0.5), math.log(8.0)))
    values = jnp.clip(jax.random.normal(value_key, (EXPERTS, RECV, D), jnp.float32), -4.0, 4.0)
    return (values * scales).astype(jnp.bfloat16)


def draw_channel_decay_rate(key, part):
    pick = jax.random.uniform(jax.random.fold_in(key, 21), (DR,), jnp.float32)
    slow = jnp.exp(jax.random.uniform(jax.random.fold_in(key, 22), (DR,), jnp.float32, math.log(0.05), math.log(0.2))) / (8.0 * TOKENS)
    fast = jnp.exp(jax.random.uniform(jax.random.fold_in(key, 23), (DR,), jnp.float32, math.log(0.003), math.log(0.01)))
    share = 0.5
    return jnp.where(pick < share, slow, fast).astype(jnp.float32)


def draw_position_extra_log_decay(key, part):
    spots = jax.random.randint(jax.random.fold_in(key, 31), (3,), 0, TOKENS)
    hit = jnp.any(jnp.arange(TOKENS)[:, None] == spots[None, :], axis=1)
    depth = jnp.log(jax.random.uniform(jax.random.fold_in(key, 32), (TOKENS,), jnp.float32, 0.5, 0.8))
    return jnp.where(hit, depth, 0.0).astype(jnp.float32)


def with_spikes(drawn, own_key, source, target, blocks, factor):
    def block_of(dim):
        return (jnp.arange(drawn.shape[dim]) // (drawn.shape[dim] // blocks)).reshape((-1,) + (1,) * (drawn.ndim - 1 - dim))

    first = jax.random.permutation(own_key, blocks)[block_of(target)]
    far = (block_of(target) + blocks // 2) % blocks
    return jnp.where((block_of(source) == first) | (block_of(source) == far), factor * drawn, drawn)


def level_of(own_key, shape, cuts, least, high):
    def one(axis_at, shards_of):
        heights = jax.random.uniform(jax.random.fold_in(jax.random.fold_in(own_key, 6), axis_at), (shards_of,), jnp.float32, least / len(cuts), high / len(cuts))
        return jnp.repeat(jnp.exp(heights), shape[axis_at] // shards_of).reshape((-1,) + (1,) * (len(shape) - axis_at - 1))

    level = one(*cuts[0])
    for cut in cuts[1:]:
        level = level * one(*cut)
    return level


def routed_block(own_key, own, number, rows, count, top, reach, skew):
    order = jax.random.permutation(own_key, count)
    heavy_load, usual = portions_of(count, rows * top, reach, skew, True), portions_of(count, rows * top, reach, skew, False)
    places = jnp.arange(count)

    def named(tallies, turn):
        used = int((tallies > 0).sum())
        fixed = max(1, used // 4)
        passed = fixed + (places - fixed + turn * (used - fixed)) % max(1, count - fixed)
        return jnp.zeros((count,), jnp.int32).at[order[jnp.where(places < fixed, places, passed)]].set(jnp.asarray(tallies, jnp.int32))

    tallies = jnp.where(number % 4 == 0, named(heavy_load, number // 4), named(usual, number - number // 4 - 1))
    mixed = jax.random.permutation(jax.random.fold_in(own, 3), count)
    giver, receiver = mixed[0:count // 2 * 2:2], mixed[1:count // 2 * 2:2]
    margin = jnp.minimum(tallies[giver] - 1, reach - tallies[receiver]) // 2
    margin = jnp.where((giver == order[0]) | (receiver == order[0]) | (tallies[receiver] == 0), 0, jnp.maximum(margin, 0))
    passed = jax.random.randint(jax.random.fold_in(own, 4), (count // 2,), 0, 1 << 20) % (margin + 1)
    tallies = tallies.at[giver].add(-passed).at[receiver].add(passed)
    members = jnp.searchsorted(jnp.cumsum(tallies), jnp.arange(rows * top), side="right").astype(jnp.int32)
    table = members.reshape(top, rows).T
    table = table[jax.random.permutation(jax.random.fold_in(own, 1), rows)]
    turn = jax.random.randint(jax.random.fold_in(own, 2), (rows, 1), 0, top)
    return jnp.take_along_axis(table, (jnp.arange(top)[None, :] + turn) % top, axis=1)


def portions_of(amount, total, most, slope, full):
    loads = [(1 << 20) // math.isqrt(grade ** slope) + 1 for grade in range(1, amount + 1)]
    largest = most if full else min(most, max(-(-total // amount), total * loads[0] // sum(loads)))
    least = 1 if total - largest >= amount - 1 else 0
    given, surplus = [largest] + [least] * (amount - 1), total - largest - least * (amount - 1)
    while surplus > 0:
        free = [i for i in range(1, amount) if given[i] < largest] or [i for i in range(1, amount) if given[i] < most]
        pool, remaining = sum([loads[i] for i in free]), surplus
        for i in free:
            addition = min(most - given[i], max(1, remaining * loads[i] // pool), surplus)
            given[i] = given[i] + addition
            surplus = surplus - addition
    return np.array(given)


def gaussian(own_key, shape, scale, bound, shards=(), kind=jnp.bfloat16):
    factor_of = level_of(own_key, shape, shards, -0.22, 0.18) if shards else 1.0
    entries = jax.random.normal(own_key, shape, jnp.float32) * scale * factor_of
    return jnp.minimum(jnp.maximum(entries, -bound), bound).astype(kind)


def bell_draw_with(stream_key, dims, deviation, limit, shards, heavy, held_as=jnp.bfloat16):
    values = deviation * jax.random.normal(stream_key, dims, jnp.float32)
    if shards:
        values = values * level_of(stream_key, dims, shards, -0.22, 0.18)
    return jnp.clip(with_spikes(values, jax.random.fold_in(stream_key, 3), *heavy), -limit, limit).astype(held_as)


def setup_inputs(seed: int = 0) -> dict:
    streams_of = jax.random.split(jax.random.key(seed), 17)
    output_cotangent = bell_draw_with(streams_of[0], (TOKENS, D), 1.0, 8.0, ((0, 32),), (0, 1, 32, 2.75))
    chosen_expert_index_keys = jax.random.split(jax.random.fold_in(streams_of[1], 1), TOKENS // TOK_DEV)
    chosen_expert_index_turns = jax.random.permutation(jax.random.fold_in(streams_of[1], 3), TOKENS // TOK_DEV)
    chosen_expert_index = jax.vmap(lambda own, number: routed_block(jax.random.fold_in(streams_of[1], 2), own, number, TOK_DEV, EXPERTS, TOP, CAP, 1))(chosen_expert_index_keys, chosen_expert_index_turns).reshape((TOKENS, TOP))
    chosen_expert_weight = jnp.clip(0.2 + 0.8 * jax.random.uniform(streams_of[2], (TOKENS, TOP), jnp.float32) ** level_of(streams_of[2], (TOKENS, TOP), ((0, 32),), -0.2, 0.2), 0.2, 1.0)
    expert_slot_tokens = draw_expert_slot_tokens(jax.random.fold_in(streams_of[16], 71), 0)
    expert_gate_matrix = gaussian(streams_of[4], (EXPERTS, D, FF), D ** -0.5, 0.125, ((0, 32), (2, 4)))
    expert_up_matrix = gaussian(streams_of[5], (EXPERTS, D, FF), D ** -0.5, 0.125, ((0, 32), (2, 4)))
    expert_down_matrix = gaussian(streams_of[6], (EXPERTS, FF, D), FF ** -0.5, 0.125, ((0, 32), (1, 4)))
    output_projection_matrix = gaussian(streams_of[7], (D, DR), DR ** -0.5, 0.125, ((1, 4),))
    recurrence_input = gaussian(streams_of[8], (TOKENS, DR), 1.0, 6.0, ((0, 32), (1, 4)))
    branch_activation_values = gaussian(streams_of[9], (TOKENS, DR), 1.0, 6.0, ((0, 32), (1, 4)))
    forward_scan_state = gaussian(streams_of[10], (TOKENS, DR), 1.0, 6.0, ((0, 32), (1, 4)), jnp.float32)
    reverse_scan_state = gaussian(streams_of[11], (TOKENS, DR), 1.0, 6.0, ((0, 32), (1, 4)), jnp.float32)
    channel_decay_rate = draw_channel_decay_rate(jax.random.fold_in(streams_of[16], 71), 0)
    position_extra_log_decay = draw_position_extra_log_decay(jax.random.fold_in(streams_of[16], 71), 0)
    recurrence_gate_weights = gaussian(streams_of[14], (BLOCKS, BW, BW), BW ** -0.5, 0.375, ((0, 4),))
    input_gate_weights = gaussian(streams_of[15], (BLOCKS, BW, BW), BW ** -0.5, 0.375, ((0, 4),))
    return dict(output_cotangent=output_cotangent, chosen_expert_index=chosen_expert_index, chosen_expert_weight=chosen_expert_weight, expert_slot_tokens=expert_slot_tokens, expert_gate_matrix=expert_gate_matrix, expert_up_matrix=expert_up_matrix, expert_down_matrix=expert_down_matrix, output_projection_matrix=output_projection_matrix, recurrence_input=recurrence_input, branch_activation_values=branch_activation_values, forward_scan_state=forward_scan_state, reverse_scan_state=reverse_scan_state, channel_decay_rate=channel_decay_rate, position_extra_log_decay=position_extra_log_decay, recurrence_gate_weights=recurrence_gate_weights, input_gate_weights=input_gate_weights)


gate_scale_factor = 8.0
clamp_limit = 7.0
glu_alpha = 1.702

def linear_prefix(coef, value):

    def combine(first, second):
        return (first[0] * second[0], second[0] * first[1] + second[1])
    return lax.associative_scan(combine, (coef, value), axis=0)[1]

def blockwise(rows, weights):
    count = rows.shape[0]
    split = rows.reshape(count, weights.shape[0], weights.shape[1]).astype(jnp.float32)
    return jnp.einsum('tbi,bij->tbj', split, weights.astype(jnp.float32)).reshape(count, -1)

def blockwise_back(rows, weights):
    count = rows.shape[0]
    split = rows.reshape(count, weights.shape[0], weights.shape[1]).astype(jnp.float32)
    return jnp.einsum('tbj,bij->tbi', split, weights.astype(jnp.float32)).reshape(count, -1)

def expert_back(items):
    tokens_in, sent_rows, w_gate, w_up, w_down = items
    gate_pre = jnp.dot(tokens_in, w_gate, preferred_element_type=jnp.float32)
    up_pre = jnp.dot(tokens_in, w_up, preferred_element_type=jnp.float32)
    glu = jnp.minimum(gate_pre, clamp_limit)
    lin = jnp.clip(up_pre, -clamp_limit, clamp_limit)
    sig = jax.nn.sigmoid(glu_alpha * glu)
    silu_part = glu * sig
    act = (silu_part * (lin + 1.0)).astype(jnp.bfloat16)
    d_act = jnp.dot(sent_rows, w_down.T, preferred_element_type=jnp.float32)
    d_glu = d_act * (lin + 1.0) * (sig + glu_alpha * silu_part * (1.0 - sig))
    d_gate = jnp.where(gate_pre < clamp_limit, d_glu, 0.0).astype(jnp.bfloat16)
    d_up = jnp.where(jnp.abs(up_pre) < clamp_limit, d_act * silu_part, 0.0).astype(jnp.bfloat16)
    down_grad = jnp.dot(act.T, sent_rows, preferred_element_type=jnp.float32).astype(jnp.bfloat16)
    gate_grad = jnp.dot(tokens_in.T, d_gate, preferred_element_type=jnp.float32).astype(jnp.bfloat16)
    up_grad = jnp.dot(tokens_in.T, d_up, preferred_element_type=jnp.float32).astype(jnp.bfloat16)
    width = FF // N_TP
    summed = jnp.zeros((tokens_in.shape[0], tokens_in.shape[1]), jnp.float32)
    for group in range(N_TP):
        low = group * width
        term = jnp.dot(d_gate[:, low:low + width], w_gate[:, low:low + width].T, preferred_element_type=jnp.float32)
        term = term + jnp.dot(d_up[:, low:low + width], w_up[:, low:low + width].T, preferred_element_type=jnp.float32)
        rounded = lax.optimization_barrier(term.astype(jnp.bfloat16))
        summed = summed + rounded.astype(jnp.float32)
    return (summed.astype(jnp.bfloat16), gate_grad, up_grad, down_grad)

def reference(output_cotangent, chosen_expert_index, chosen_expert_weight, expert_slot_tokens, expert_gate_matrix, expert_up_matrix, expert_down_matrix, output_projection_matrix, recurrence_input, branch_activation_values, forward_scan_state, reverse_scan_state, channel_decay_rate, position_extra_log_decay, recurrence_gate_weights, input_gate_weights):
    pairs = TOKENS * TOP
    assigned = chosen_expert_index.reshape(N_SP, TOK_DEV * TOP)
    onehot = (assigned[:, :, None] == jnp.arange(EXPERTS, dtype=jnp.int32)[None, None, :]).astype(jnp.int32)
    before = jnp.cumsum(onehot, axis=1) - onehot
    slot = lax.optimization_barrier(jnp.sum(before * onehot, axis=2))
    source = jnp.arange(N_SP, dtype=jnp.int32)[:, None]
    target = (assigned * RECV + source * CAP + slot).reshape(-1).astype(jnp.int32)
    owner = jnp.full((EXPERTS * RECV,), pairs, jnp.int32).at[target].set(jnp.arange(pairs, dtype=jnp.int32))
    weighted = (chosen_expert_weight[:, :, None] * output_cotangent.astype(jnp.float32)[:, None, :]).astype(jnp.bfloat16)
    padded = jnp.concatenate([weighted.reshape(pairs, D), jnp.zeros((1, D), jnp.bfloat16)], axis=0)
    sent = jnp.take(padded, owner, axis=0).reshape(EXPERTS, RECV, D)
    back, gate_grad, up_grad, down_grad = lax.map(expert_back, (expert_slot_tokens, sent, expert_gate_matrix, expert_up_matrix, expert_down_matrix))
    rows = jnp.take(back.reshape(EXPERTS * RECV, D), target, axis=0).astype(jnp.float32)
    z_grad = (output_cotangent.astype(jnp.float32) + lax.optimization_barrier(jnp.sum(rows.reshape(TOKENS, TOP, D), axis=1))).astype(jnp.bfloat16)
    recurrence_gate_value = jax.nn.sigmoid(blockwise(recurrence_input, recurrence_gate_weights))
    inp = jax.nn.sigmoid(blockwise(recurrence_input, input_gate_weights))
    log_decay_factor = -gate_scale_factor * recurrence_gate_value * channel_decay_rate[None, :] + position_extra_log_decay[:, None]
    decay = jnp.exp(log_decay_factor)
    scale_in = jnp.sqrt(-jnp.expm1(2.0 * log_decay_factor))
    inputs = recurrence_input.astype(jnp.float32)
    xin = scale_in * inp * inputs
    forward_state = decay * forward_scan_state + xin
    backward_state = decay * reverse_scan_state + xin
    mixed_state = (forward_state + backward_state).astype(jnp.bfloat16)
    branch = branch_activation_values.astype(jnp.float32)
    gated = (mixed_state.astype(jnp.float32) * branch).astype(jnp.bfloat16)
    proj_grad = jnp.dot(z_grad.T, gated, preferred_element_type=jnp.float32)
    d_gated = jnp.dot(z_grad, output_projection_matrix, preferred_element_type=jnp.float32)
    branch_grad = (d_gated * mixed_state.astype(jnp.float32)).astype(jnp.bfloat16)
    d_state = d_gated * branch
    zero_row = jnp.zeros((1, DR), jnp.float32)
    later = jnp.flip(linear_prefix(jnp.flip(jnp.concatenate([decay[1:], zero_row], axis=0), 0), jnp.flip(d_state, 0)), 0)
    earlier = linear_prefix(jnp.concatenate([zero_row, decay[:-1]], axis=0), d_state)
    total = later + earlier
    d_log_a = (later * forward_scan_state + earlier * reverse_scan_state) * decay - total * inp * inputs * decay * decay / scale_in
    rec_pre_grad = (d_log_a * (-gate_scale_factor * channel_decay_rate[None, :]) * recurrence_gate_value * (1.0 - recurrence_gate_value)).astype(jnp.bfloat16)
    inp_pre_grad = (total * scale_in * inputs * inp * (1.0 - inp)).astype(jnp.bfloat16)
    input_grad = (total * scale_in * inp + blockwise_back(rec_pre_grad, recurrence_gate_weights) + blockwise_back(inp_pre_grad, input_gate_weights)).astype(jnp.bfloat16)
    return (gate_grad, up_grad, down_grad, proj_grad, branch_grad, input_grad)
```

```python
import functools

import jax
import jax.numpy as jnp
from jax import lax
from jax.experimental import pallas as pl
from jax.experimental.pallas import tpu as pltpu
from jax.sharding import PartitionSpec as P


gate_scale_factor = 8.0
clamp_limit = 7.0
glu_alpha = 1.702

BF = jnp.bfloat16
F32 = jnp.float32

SLOT_GROUPS = (24, 16)

ROWS_ROWS = (((1,), (1,)), ((), ()))
COLS_COLS = (((0,), (0,)), ((), ()))


def params(limit_mib=48):
    return pltpu.CompilerParams(vmem_limit_bytes=limit_mib * 1024 * 1024)


def iota(shape, dim):
    return lax.broadcasted_iota(jnp.int32, shape, dim)


def placed_row(expert, slot, experts):
    base, row = 0, None
    for size in SLOT_GROUPS:
        here = base * experts + expert * size + (slot - base)
        row = here if row is None else jnp.where(slot >= base, here, row)
        base += size
    return row


def slots_kernel(idx_ref, idx_t_ref, col_ref, row_ref, *, experts):
    tokens, top = idx_ref.shape
    a, b = iota((tokens, tokens), 0), iota((tokens, tokens), 1)
    hot = [idx_ref[:, k : k + 1] == iota((tokens, experts), 1) for k in range(top)]
    both = sum(h.astype(F32) for h in hot).astype(BF)
    before = jnp.dot((b < a).astype(F32).astype(BF), both, preferred_element_type=F32)
    for k in range(top):
        rank = jnp.sum(jnp.where(hot[k], before, 0.0), axis=1, keepdims=True).astype(jnp.int32)
        col_ref[:, k : k + 1] = placed_row(idx_ref[:, k : k + 1], rank, experts)
    hot = [idx_t_ref[k : k + 1, :] == iota((experts, tokens), 0) for k in range(top)]
    both = sum(h.astype(F32) for h in hot).astype(BF)
    before = jnp.dot(both, (a < b).astype(F32).astype(BF), preferred_element_type=F32)
    for k in range(top):
        rank = jnp.sum(jnp.where(hot[k], before, 0.0), axis=0, keepdims=True).astype(jnp.int32)
        row_ref[k : k + 1, :] = placed_row(idx_t_ref[k : k + 1, :], rank, experts)


def slot_rows(chosen, experts):
    tokens, top = chosen.shape
    return pl.pallas_call(
        functools.partial(slots_kernel, experts=experts),
        out_shape=(
            jax.ShapeDtypeStruct((tokens, top), jnp.int32),
            jax.ShapeDtypeStruct((top, tokens), jnp.int32),
        ),
        compiler_params=params(),
        name="slots",
    )(chosen, chosen.T)


def dispatch_kernel(row_ref, weight_ref, cot_ref, out_ref, *, first):
    rows, tokens = out_ref.shape[0], cot_ref.shape[0]
    at = first + pl.program_id(0) * rows + iota((rows, tokens), 0)
    weight = jnp.zeros((rows, tokens), F32)
    for k in range(row_ref.shape[0]):
        weight = jnp.where(row_ref[k : k + 1, :] == at, weight_ref[k : k + 1, :], weight)
    picked = jnp.dot((weight > 0.0).astype(F32).astype(BF), cot_ref[...], preferred_element_type=F32)
    out_ref[...] = (picked * jnp.sum(weight, axis=1, keepdims=True)).astype(BF)


def dispatch(row, weight_t, cot, first, count):
    _, width = cot.shape
    block = 128
    return pl.pallas_call(
        functools.partial(dispatch_kernel, first=first),
        grid=(count // block,),
        in_specs=[
            pl.BlockSpec(row.shape, lambda i: (0, 0)),
            pl.BlockSpec(weight_t.shape, lambda i: (0, 0)),
            pl.BlockSpec(cot.shape, lambda i: (0, 0)),
        ],
        out_specs=pl.BlockSpec((block, width), lambda i: (i, 0)),
        out_shape=jax.ShapeDtypeStruct((count, width), BF),
        compiler_params=params(),
        name="dispatch",
    )(row, weight_t, cot)


def forward_kernel(x_ref, gate_ref, up_ref, act_ref, slope_ref):
    x = x_ref[...]
    hidden = gate_ref.shape[1]
    gate_pre = jnp.dot(x, gate_ref[...], preferred_element_type=F32)
    up_pre = jnp.dot(x, up_ref[...], preferred_element_type=F32)
    glu = jnp.minimum(gate_pre, clamp_limit)
    lin = jnp.clip(up_pre, -clamp_limit, clamp_limit) + 1.0
    sig = 1.0 / (1.0 + jnp.exp(-glu_alpha * glu))
    silu = glu * sig
    act_ref[...] = (silu * lin).astype(BF)
    slope = lin * (sig + glu_alpha * silu * (1.0 - sig))
    slope_ref[:, :hidden] = jnp.where(gate_pre < clamp_limit, slope, 0.0)
    slope_ref[:, hidden:] = jnp.where(jnp.abs(up_pre) < clamp_limit, silu, 0.0)


def expert_forward(x, w_gate, w_up):
    rows, width = x.shape
    hidden = w_gate.shape[1]
    block = 256
    whole = pl.BlockSpec((width, hidden), lambda i: (0, 0))
    return pl.pallas_call(
        forward_kernel,
        grid=(rows // block,),
        in_specs=[pl.BlockSpec((block, width), lambda i: (i, 0)), whole, whole],
        out_specs=(
            pl.BlockSpec((block, hidden), lambda i: (i, 0)),
            pl.BlockSpec((block, 2 * hidden), lambda i: (i, 0)),
        ),
        out_shape=(
            jax.ShapeDtypeStruct((rows, hidden), BF),
            jax.ShapeDtypeStruct((rows, 2 * hidden), F32),
        ),
        compiler_params=params(),
        name="expert_forward",
    )(x, w_gate, w_up)


def backward_kernel(
    rank_ref,
    got_ref,
    slope_ref,
    down_ref,
    gate_hbm,
    up_hbm,
    both_ref,
    up1_ref,
    dn1_ref,
    up2_ref,
    dn2_ref,
    mine_ref,
    gate_ref,
    up_ref,
    sems,
    *,
    n_tp,
):
    half = got_ref.shape[0] // 2
    hidden = down_ref.shape[0]
    width = mine_ref.shape[1]
    copies = [
        pltpu.make_async_copy(gate_hbm, gate_ref, sems.at[0]),
        pltpu.make_async_copy(up_hbm, up_ref, sems.at[1]),
    ]
    for copy in copies:
        copy.start()
    d_act = lax.dot_general(got_ref[...], down_ref[...], ROWS_ROWS, preferred_element_type=F32)
    d_gate = (d_act * slope_ref[:, :hidden]).astype(BF)
    d_up = (d_act * slope_ref[:, hidden:]).astype(BF)
    both_ref[:, :hidden] = d_gate
    both_ref[:, hidden:] = d_up
    for copy in copies:
        copy.wait()

    def term(ahead):
        at = pl.multiple_of(lax.rem(rank_ref[0] + ahead, n_tp) * width, width)
        both = lax.dot_general(
            d_gate, gate_ref[pl.ds(at, width), :], ROWS_ROWS, preferred_element_type=F32
        )
        both = both + lax.dot_general(
            d_up, up_ref[pl.ds(at, width), :], ROWS_ROWS, preferred_element_type=F32
        )
        return both.astype(BF)

    away = term(2)
    up1_ref[:half, :] = away[:half]
    dn1_ref[:half, :] = away[half:]
    above = term(1)
    up1_ref[half:, :] = above[half:]
    up2_ref[...] = above[:half]
    below = term(3)
    dn1_ref[half:, :] = below[:half]
    dn2_ref[...] = below[half:]
    mine_ref[...] = term(0)


def expert_backward(rank, got, slope, w_down, w_gate, w_up, n_tp):
    rows, width = got.shape
    hidden = w_down.shape[0]
    part = width // n_tp
    full = lambda a, b: pl.BlockSpec((a, b), lambda i: (0, 0))
    outs = [
        (rows, 2 * hidden),
        (rows, part),
        (rows, part),
        (rows // 2, part),
        (rows // 2, part),
        (rows, part),
    ]
    return pl.pallas_call(
        functools.partial(backward_kernel, n_tp=n_tp),
        grid=(1,),
        in_specs=[
            pl.BlockSpec(memory_space=pltpu.SMEM),
            full(rows, width),
            full(rows, 2 * hidden),
            full(hidden, width),
            pl.BlockSpec(memory_space=pl.ANY),
            pl.BlockSpec(memory_space=pl.ANY),
        ],
        out_specs=tuple(full(*s) for s in outs),
        out_shape=tuple(jax.ShapeDtypeStruct(s, BF) for s in outs),
        scratch_shapes=[
            pltpu.VMEM(w_gate.shape, BF),
            pltpu.VMEM(w_up.shape, BF),
            pltpu.SemaphoreType.DMA((2,)),
        ],
        compiler_params=params(),
        name="expert_backward",
    )(rank, got, slope, w_down, w_gate, w_up)


def summed_products(lefts, rights):
    total = None
    for left, right in zip(lefts, rights):
        term = lax.dot_general(left[...], right[...], COLS_COLS, preferred_element_type=F32)
        total = term if total is None else total + term
    return total


def gate_up_kernel(*refs, groups):
    gate_ref, up_ref = refs[2 * groups :]
    total = summed_products(refs[:groups], refs[groups : 2 * groups])
    hidden = gate_ref.shape[1]
    gate_ref[...] = total[:, :hidden].astype(BF)
    up_ref[...] = total[:, hidden:].astype(BF)


def gate_up_grads(saved, both):
    width, hidden = saved[0].shape[1], both[0].shape[1] // 2
    block = 256
    out = pl.BlockSpec((block, hidden), lambda i: (i, 0))
    return pl.pallas_call(
        functools.partial(gate_up_kernel, groups=len(saved)),
        grid=(width // block,),
        in_specs=[pl.BlockSpec((x.shape[0], block), lambda i: (0, i)) for x in saved]
        + [pl.BlockSpec(g.shape, lambda i: (0, 0)) for g in both],
        out_specs=(out, out),
        out_shape=(jax.ShapeDtypeStruct((width, hidden), BF),) * 2,
        compiler_params=params(),
        name="gate_up_grads",
    )(*saved, *both)


def down_kernel(*refs, groups):
    refs[-1][...] = summed_products(refs[:groups], refs[groups : 2 * groups]).astype(BF)


def down_grads(acts, gots):
    width, hidden = gots[0].shape[1], acts[0].shape[1]
    block = 512
    return pl.pallas_call(
        functools.partial(down_kernel, groups=len(acts)),
        grid=(width // block,),
        in_specs=[pl.BlockSpec(a.shape, lambda i: (0, 0)) for a in acts]
        + [pl.BlockSpec((g.shape[0], block), lambda i: (0, i)) for g in gots],
        out_specs=pl.BlockSpec((hidden, block), lambda i: (0, i)),
        out_shape=jax.ShapeDtypeStruct((hidden, width), BF),
        compiler_params=params(),
        name="down_grads",
    )(*acts, *gots)


def ring(n, step):
    return [(i, (i + step) % n) for i in range(n)]


def summed_over_tp(up1, dn1, up2, dn2, mine, n_tp):
    half = up2.shape[0]
    from_below = lax.ppermute(up1, "tp", ring(n_tp, 1))
    from_above = lax.ppermute(dn1, "tp", ring(n_tp, -1))
    add = lambda a, b: (a.astype(F32) + b.astype(F32)).astype(BF)
    up2 = add(up2, from_below[:half])
    dn2 = add(dn2, from_above[:half])
    top = lax.ppermute(up2, "tp", ring(n_tp, 1))
    bottom = lax.ppermute(dn2, "tp", ring(n_tp, -1))
    upper = (
        mine[:half].astype(F32) + top.astype(F32) + from_above[half:].astype(F32)
    ).astype(BF)
    lower = (
        mine[half:].astype(F32) + bottom.astype(F32) + from_below[half:].astype(F32)
    ).astype(BF)
    return jnp.concatenate([upper, lower], axis=0)


def combine_kernel(col_ref, cot_ref, *refs):
    back_refs, out_ref = refs[:-1], refs[-1]
    tokens, top = col_ref.shape
    total, first = None, 0
    for back_ref in back_refs:
        rows = back_ref.shape[0]
        at = first + iota((tokens, rows), 1)
        hit = col_ref[:, 0:1] == at
        for k in range(1, top):
            hit = hit | (col_ref[:, k : k + 1] == at)
        term = jnp.dot(hit.astype(F32).astype(BF), back_ref[...], preferred_element_type=F32)
        total = term if total is None else total + term
        first += rows
    out_ref[...] = (cot_ref[...].astype(F32) + total).astype(BF)


def combine(col, cot_part, backs):
    return pl.pallas_call(
        combine_kernel,
        out_shape=jax.ShapeDtypeStruct(cot_part.shape, BF),
        compiler_params=params(),
        name="combine",
    )(col, cot_part, *backs)


def pieces_of(rank_ref, z_refs, n_tp):
    z0, z_below, z_above, z_top, z_bottom = z_refs
    me = rank_ref[0]
    away = jnp.concatenate([z_top[...], z_bottom[...]], axis=0)
    order = ((0, z0[...]), (n_tp - 1, z_below[...]), (1, z_above[...]), (2, away))
    width = z0.shape[1]
    return [(pl.multiple_of(lax.rem(me + a, n_tp) * width, width), z) for a, z in order]


def state_kernel(
    rank_ref,
    z0,
    z1,
    z2,
    z3,
    z4,
    w_hbm,
    mixed_ref,
    branch_ref,
    decay_ref,
    later_ref,
    earlier_ref,
    branch_grad_ref,
    state_ref,
    carry_ref,
    w_ref,
    sem,
    *,
    n_tp,
):
    copy = pltpu.make_async_copy(w_hbm, w_ref, sem)
    copy.start()
    copy.wait()
    total = None
    for at, z in pieces_of(rank_ref, (z0, z1, z2, z3, z4), n_tp):
        term = jnp.dot(z, w_ref[pl.ds(at, z.shape[1]), :], preferred_element_type=F32)
        total = term if total is None else total + term
    branch_grad_ref[...] = (total * mixed_ref[...].astype(F32)).astype(BF)
    state = total * branch_ref[...].astype(F32)
    state_ref[...] = state
    scaled = state * decay_ref[...]
    ahead = jnp.sum(scaled * earlier_ref[...], axis=0, keepdims=True)
    behind = jnp.sum(scaled * later_ref[...], axis=0, keepdims=True)
    last = slice(state.shape[0] - 1, state.shape[0])
    through = decay_ref[last, :] * earlier_ref[last, :]
    lanes = carry_ref.shape[2]
    count = ahead.shape[1] // lanes
    tile = jnp.concatenate(
        [
            v[:, b * lanes : (b + 1) * lanes]
            for v in (ahead, behind, through, through)
            for b in range(count)
        ],
        axis=0,
    )
    carry_ref[...] = jnp.broadcast_to(tile[None], carry_ref.shape)


def state_grads(rank, zs, w_out, mixed, branch, decay, later_prod, earlier_prod, n_sp, n_tp):
    tokens, channels = mixed.shape
    return pl.pallas_call(
        functools.partial(state_kernel, n_tp=n_tp),
        in_specs=[pl.BlockSpec(memory_space=pltpu.SMEM)]
        + [pl.BlockSpec(memory_space=pltpu.VMEM)] * 5
        + [pl.BlockSpec(memory_space=pl.ANY)]
        + [pl.BlockSpec(memory_space=pltpu.VMEM)] * 5,
        out_shape=(
            jax.ShapeDtypeStruct((tokens, channels), BF),
            jax.ShapeDtypeStruct((tokens, channels), F32),
            jax.ShapeDtypeStruct((n_sp, 16, channels // 4), F32),
        ),
        scratch_shapes=[pltpu.VMEM(w_out.shape, BF), pltpu.SemaphoreType.DMA(())],
        compiler_params=params(),
        name="state_grads",
    )(rank, *zs, w_out, mixed, branch, decay, later_prod, earlier_prod)


def proj_kernel(rank_ref, core_ref, z0, z1, z2, z3, z4, gated_ref, keep_ref, send_ref, *, n_tp, size):
    gated = gated_ref[...]
    odd = core_ref[0] == 1
    for at, z in pieces_of(rank_ref, (z0, z1, z2, z3, z4), n_tp):
        term = lax.dot_general(z, gated, COLS_COLS, preferred_element_type=F32).astype(BF)
        for i in range(term.shape[0] // (2 * size)):
            first = term[2 * i * size : (2 * i + 1) * size]
            second = term[(2 * i + 1) * size : (2 * i + 2) * size]
            rows = pl.ds(pl.multiple_of(at // 2, size) + i * size, size)
            keep_ref[rows, :] = jnp.where(odd, second, first)
            send_ref[rows, :] = jnp.where(odd, first, second)


def proj_terms(rank, core, zs, gated, n_tp, n_sp):
    width = zs[0].shape[1] * n_tp
    half = jax.ShapeDtypeStruct((width // 2, gated.shape[1]), BF)
    return pl.pallas_call(
        functools.partial(proj_kernel, n_tp=n_tp, size=width // n_sp),
        in_specs=[pl.BlockSpec(memory_space=pltpu.SMEM)] * 2
        + [pl.BlockSpec(memory_space=pltpu.VMEM)] * 6,
        out_shape=(half, half),
        compiler_params=params(),
        name="proj_terms",
    )(rank, core, *zs, gated)


def scan_kernel(state_ref, decay_ref, later_ref, earlier_ref):
    rows, channels = state_ref.shape
    zero = jnp.zeros((1, channels), F32)

    def step(i, carry):
        ahead, behind = carry
        t = rows - 1 - i
        later = state_ref[pl.ds(t, 1), :] + ahead
        later_ref[pl.ds(t, 1), :] = later
        earlier = state_ref[pl.ds(i, 1), :] + behind
        earlier_ref[pl.ds(i, 1), :] = earlier
        return (later * decay_ref[pl.ds(t, 1), :], earlier * decay_ref[pl.ds(i, 1), :])

    lax.fori_loop(0, rows, step, (zero, zero), unroll=8)


def local_scans(state, decay):
    return pl.pallas_call(
        scan_kernel,
        out_shape=(
            jax.ShapeDtypeStruct(state.shape, F32),
            jax.ShapeDtypeStruct(state.shape, F32),
        ),
        compiler_params=params(),
        name="local_scans",
    )(state, decay)


def carried_in(me, got_ref):
    count, half = got_ref.shape[0], got_ref.shape[1] // 2
    carry = lambda q: got_ref[q, :half, :]
    through = lambda q: got_ref[q, half:, :]
    zero = jnp.zeros((half, got_ref.shape[2]), F32)
    ahead, behind = zero, zero
    for q in range(count):
        p = count - 1 - q
        ahead = jnp.where(p > me, carry(p) + through(p) * ahead, ahead)
        behind = jnp.where(q < me, carry(q) + through(q) * behind, behind)
    return ahead[: half // 2], behind[half // 2 :]


def final_kernel(
    me_ref,
    got_ref,
    later_ref,
    earlier_ref,
    later_prod,
    earlier_prod,
    h_later,
    h_earlier,
    q_ref,
    r_ref,
    rec_w,
    inp_w,
    out_ref,
):
    ahead, behind = carried_in(me_ref[0], got_ref)
    spread = lambda v: jnp.concatenate([v[b : b + 1] for b in range(v.shape[0])], axis=1)
    later = later_ref[...] + later_prod[...] * spread(ahead)
    earlier = earlier_ref[...] + earlier_prod[...] * spread(behind)
    total = later + earlier
    rec_pre = (later * h_later[...] + earlier * h_earlier[...]).astype(BF)
    inp_pre = (total * q_ref[...]).astype(BF)
    direct = total * r_ref[...]
    size = rec_w.shape[1]
    for b in range(rec_w.shape[0]):
        cols = slice(b * size, (b + 1) * size)
        term = lax.dot_general(rec_pre[:, cols], rec_w[b], ROWS_ROWS, preferred_element_type=F32)
        term = term + lax.dot_general(
            inp_pre[:, cols], inp_w[b], ROWS_ROWS, preferred_element_type=F32
        )
        out_ref[:, cols] = (direct[:, cols] + term).astype(BF)


def final_grads(me, got, arrays, rec_w, inp_w):
    tokens, channels = arrays[0].shape
    return pl.pallas_call(
        final_kernel,
        in_specs=[pl.BlockSpec(memory_space=pltpu.SMEM)]
        + [pl.BlockSpec(memory_space=pltpu.VMEM)] * 11,
        out_shape=jax.ShapeDtypeStruct((tokens, channels), BF),
        compiler_params=params(),
        name="final_grads",
    )(me, got, *arrays, rec_w, inp_w)


def blockwise(rows, weights):
    size = weights.shape[1]
    return jnp.concatenate(
        [
            jnp.dot(rows[:, b * size : (b + 1) * size], weights[b], preferred_element_type=F32)
            for b in range(weights.shape[0])
        ],
        axis=1,
    )


def shards(
    output_cotangent,
    chosen_expert_index,
    chosen_expert_weight,
    expert_slot_tokens,
    expert_gate_matrix,
    expert_up_matrix,
    expert_down_matrix,
    output_projection_matrix,
    recurrence_input,
    branch_activation_values,
    forward_scan_state,
    reverse_scan_state,
    channel_decay_rate,
    position_extra_log_decay,
    recurrence_gate_weights,
    input_gate_weights,
):
    n_sp = lax.axis_size("sp")
    n_tp = lax.axis_size("tp")
    tokens, model_width = output_cotangent.shape
    experts = n_sp * expert_gate_matrix.shape[0]
    capacity = expert_slot_tokens.shape[1] // n_sp
    part = model_width // n_tp
    rank = lax.axis_index("tp").astype(jnp.int32).reshape(1)
    place = lax.axis_index("sp").astype(jnp.int32).reshape(1)
    bounds, at = [], 0
    for size in SLOT_GROUPS:
        bounds.append((at, size))
        at += size

    col, row = slot_rows(chosen_expert_index, experts)
    weight_t = chosen_expert_weight.T
    received = []
    for base, size in bounds:
        out = dispatch(row, weight_t, output_cotangent, base * experts, size * experts)
        out = out.reshape(experts, size, model_width)
        got = lax.all_to_all(out, "sp", 0, 0, tiled=True)
        received.append(got.reshape(n_sp * size, model_width))

    w_gate, w_up, w_down = expert_gate_matrix[0], expert_up_matrix[0], expert_down_matrix[0]
    by_source = expert_slot_tokens.reshape(n_sp, capacity, model_width)
    saved, acts, slopes = [], [], []
    for base, size in bounds:
        x = by_source[:, base : base + size].reshape(n_sp * size, model_width)
        act, slope = expert_forward(x, w_gate, w_up)
        saved.append(x)
        acts.append(act)
        slopes.append(slope)

    rec = jax.nn.sigmoid(blockwise(recurrence_input, recurrence_gate_weights))
    inp = jax.nn.sigmoid(blockwise(recurrence_input, input_gate_weights))
    rate = -gate_scale_factor * channel_decay_rate[None, :]
    log_decay = rec * rate + position_extra_log_decay[:, None]
    decay = jnp.exp(log_decay)
    scale_in = jnp.sqrt(-jnp.expm1(2.0 * log_decay))
    inputs = recurrence_input.astype(F32)
    xin = scale_in * inp * inputs
    mixed = (
        (decay * forward_scan_state + xin) + (decay * reverse_scan_state + xin)
    ).astype(BF)
    gated = (mixed.astype(F32) * branch_activation_values.astype(F32)).astype(BF)
    lower = (iota((tokens, tokens), 1) <= iota((tokens, tokens), 0)).astype(F32)
    running = jnp.dot(lower, log_decay, precision=lax.Precision.HIGHEST)
    later_prod = jnp.exp(running[-1:] - running)
    earlier_prod = jnp.exp(running - log_decay)
    rec_slope = rate * rec * (1.0 - rec)
    shared = inp * inputs * decay * decay / scale_in
    h_later = (forward_scan_state * decay - shared) * rec_slope
    h_earlier = (reverse_scan_state * decay - shared) * rec_slope
    q = scale_in * inputs * inp * (1.0 - inp)
    r = scale_in * inp
    cot_part = lax.dynamic_slice_in_dim(output_cotangent, rank[0] * part, part, 1)

    boths, backs = [], []
    for g, ((base, size), got) in enumerate(zip(bounds, received)):
        both, *terms = expert_backward(rank, got, slopes[g], w_down, w_gate, w_up, n_tp)
        summed = summed_over_tp(*terms, n_tp)
        back = lax.all_to_all(summed.reshape(n_sp, size, part), "sp", 0, 0, tiled=True)
        backs.append(back.reshape(experts * size, part))
        boths.append(both)
    gate_grad, up_grad = gate_up_grads(saved, boths)
    down_grad = down_grads(acts, received)

    z0 = combine(col, cot_part, backs)
    z_below = lax.ppermute(z0, "tp", ring(n_tp, 1))
    z_above = lax.ppermute(z0, "tp", ring(n_tp, -1))
    z_top = lax.ppermute(z_below[: tokens // 2], "tp", ring(n_tp, 1))
    z_bottom = lax.ppermute(z_above[tokens // 2 :], "tp", ring(n_tp, -1))
    zs = (z0, z_below, z_above, z_top, z_bottom)

    branch_grad, state, carry = state_grads(
        rank,
        zs,
        output_projection_matrix,
        mixed,
        branch_activation_values,
        decay,
        later_prod,
        earlier_prod,
        n_sp,
        n_tp,
    )
    carried = lax.all_to_all(carry, "sp", 0, 0, tiled=True)
    keep, send = proj_terms(rank, place % 2, zs, gated, n_tp, n_sp)
    other = lax.ppermute(send, "sp", [(i, i ^ 1) for i in range(n_sp)])
    terms = (keep.astype(F32) + other.astype(F32)).astype(BF)
    terms = terms.reshape(n_sp // 2, model_width // n_sp, -1)
    groups = [list(range(c, n_sp, 2)) for c in range(2)]
    terms = lax.all_to_all(terms, "sp", 0, 0, axis_index_groups=groups, tiled=True)
    later, earlier = local_scans(state, decay)
    input_grad = final_grads(
        place,
        carried,
        (later, earlier, later_prod, earlier_prod, h_later, h_earlier, q, r),
        recurrence_gate_weights,
        input_gate_weights,
    )
    proj_grad = jnp.sum(terms.astype(F32), axis=0)
    return (gate_grad[None], up_grad[None], down_grad[None], proj_grad, branch_grad, input_grad)


def solution(mesh):
    in_specs = (
        P("sp", None),
        P("sp", None),
        P("sp", None),
        P("sp", None, None),
        P("sp", None, "tp"),
        P("sp", None, "tp"),
        P("sp", "tp", None),
        P(None, "tp"),
        P("sp", "tp"),
        P("sp", "tp"),
        P("sp", "tp"),
        P("sp", "tp"),
        P("tp"),
        P("sp"),
        P("tp", None, None),
        P("tp", None, None),
    )
    out_specs = (
        P("sp", None, "tp"),
        P("sp", None, "tp"),
        P("sp", "tp", None),
        P("sp", "tp"),
        P("sp", "tp"),
        P("sp", "tp"),
    )
    return jax.shard_map(shards, mesh=mesh, in_specs=in_specs, out_specs=out_specs, check_vma=False)
```

```python
import functools

import jax
import jax.numpy as jnp
from jax import lax
from jax.experimental import pallas as pl
from jax.experimental.pallas import tpu as pltpu
from jax.sharding import PartitionSpec as P


gate_scale_factor = 8.0
clamp_limit = 7.0
glu_alpha = 1.702

BF = jnp.bfloat16
F32 = jnp.float32

SLOT_GROUPS = (24, 16)

ROWS_ROWS = (((1,), (1,)), ((), ()))
COLS_COLS = (((0,), (0,)), ((), ()))


def params(limit_mib):
    return pltpu.CompilerParams(vmem_limit_bytes=limit_mib * 1024 * 1024)


def hbm(shape, dtype=BF):
    return pltpu.HBM(shape, dtype)


def in_hbm(*arrays):
    return tuple(pltpu.with_memory_space_constraint(a, pltpu.HBM) for a in arrays)


def iota(shape, dim):
    return lax.broadcasted_iota(jnp.int32, shape, dim)


def placed_row(expert, slot, experts):
    base, row = 0, None
    for size in SLOT_GROUPS:
        here = base * experts + expert * size + (slot - base)
        row = here if row is None else jnp.where(slot >= base, here, row)
        base += size
    return row


def slots_kernel(idx_ref, idx_t_ref, col_ref, row_ref, *, experts):
    tokens, top = idx_ref.shape
    a, b = iota((tokens, tokens), 0), iota((tokens, tokens), 1)
    hot = [idx_ref[:, k : k + 1] == iota((tokens, experts), 1) for k in range(top)]
    both = sum(h.astype(F32) for h in hot).astype(BF)
    before = jnp.dot((b < a).astype(F32).astype(BF), both, preferred_element_type=F32)
    for k in range(top):
        rank = jnp.sum(jnp.where(hot[k], before, 0.0), axis=1, keepdims=True).astype(jnp.int32)
        col_ref[:, k : k + 1] = idx_ref[:, k : k + 1] * sum(SLOT_GROUPS) + rank
    hot = [idx_t_ref[k : k + 1, :] == iota((experts, tokens), 0) for k in range(top)]
    both = sum(h.astype(F32) for h in hot).astype(BF)
    before = jnp.dot(both, (a < b).astype(F32).astype(BF), preferred_element_type=F32)
    for k in range(top):
        rank = jnp.sum(jnp.where(hot[k], before, 0.0), axis=0, keepdims=True).astype(jnp.int32)
        row_ref[k : k + 1, :] = placed_row(idx_t_ref[k : k + 1, :], rank, experts)


def slot_rows(chosen, experts):
    tokens, top = chosen.shape
    return pl.pallas_call(
        functools.partial(slots_kernel, experts=experts),
        out_shape=(
            jax.ShapeDtypeStruct((tokens, top), jnp.int32),
            jax.ShapeDtypeStruct((top, tokens), jnp.int32),
        ),
        compiler_params=params(8),
        name="slots",
    )(chosen, chosen.T)


def dispatch_kernel(row_ref, weight_ref, cot_ref, out_ref, *, first):
    rows, tokens = out_ref.shape[0], cot_ref.shape[0]
    at = first + pl.program_id(0) * rows + iota((rows, tokens), 0)
    weight = jnp.zeros((rows, tokens), F32)
    for k in range(row_ref.shape[0]):
        weight = jnp.where(row_ref[k : k + 1, :] == at, weight_ref[k : k + 1, :], weight)
    picked = jnp.dot((weight > 0.0).astype(F32).astype(BF), cot_ref[...], preferred_element_type=F32)
    out_ref[...] = (picked * jnp.sum(weight, axis=1, keepdims=True)).astype(BF)


def dispatch(row, weight_t, cot, first, count):
    _, width = cot.shape
    block = 256
    return pl.pallas_call(
        functools.partial(dispatch_kernel, first=first),
        grid=(count // block,),
        in_specs=[
            pl.BlockSpec(row.shape, lambda i: (0, 0)),
            pl.BlockSpec(weight_t.shape, lambda i: (0, 0)),
            pl.BlockSpec(cot.shape, lambda i: (0, 0)),
        ],
        out_specs=pl.BlockSpec((block, width), lambda i: (i, 0)),
        out_shape=hbm((count, width)),
        compiler_params=params(10),
        name="dispatch",
    )(row, weight_t, cot)


def hold_kernel(*refs):
    count = len(refs) // 2
    sems = refs[-1]
    copies = [
        pltpu.make_async_copy(refs[i], refs[count + i], sems.at[i]) for i in range(count)
    ]
    for copy in copies:
        copy.start()
    for copy in copies:
        copy.wait()


def held(*arrays):
    return pl.pallas_call(
        hold_kernel,
        in_specs=[pl.BlockSpec(memory_space=pl.ANY)] * len(arrays),
        out_specs=tuple([pl.BlockSpec(memory_space=pltpu.VMEM)] * len(arrays)),
        out_shape=tuple(pltpu.VMEM(a.shape, a.dtype) for a in arrays),
        scratch_shapes=[pltpu.SemaphoreType.DMA((len(arrays),))],
        compiler_params=params(4),
        name="fetch",
    )(*in_hbm(*arrays))


def forward_kernel(x_ref, gate_ref, up_ref, act_ref, slope_ref):
    x = x_ref[...]
    hidden = gate_ref.shape[1]
    gate_pre = jnp.dot(x, gate_ref[...], preferred_element_type=F32)
    up_pre = jnp.dot(x, up_ref[...], preferred_element_type=F32)
    glu = jnp.minimum(gate_pre, clamp_limit)
    lin = jnp.clip(up_pre, -clamp_limit, clamp_limit) + 1.0
    sig = 1.0 / (1.0 + jnp.exp(-glu_alpha * glu))
    silu = glu * sig
    act_ref[...] = (silu * lin).astype(BF)
    slope = lin * (sig + glu_alpha * silu * (1.0 - sig))
    slope_ref[:, :hidden] = jnp.where(gate_pre < clamp_limit, slope, 0.0)
    slope_ref[:, hidden:] = jnp.where(jnp.abs(up_pre) < clamp_limit, silu, 0.0)


def expert_forward(x, w_gate, w_up):
    rows, width = x.shape
    hidden = w_gate.shape[1]
    block = 256
    whole = pl.BlockSpec(memory_space=pltpu.VMEM)
    return pl.pallas_call(
        forward_kernel,
        grid=(rows // block,),
        in_specs=[pl.BlockSpec((block, width), lambda i: (i, 0)), whole, whole],
        out_specs=(
            pl.BlockSpec((block, hidden), lambda i: (i, 0)),
            pl.BlockSpec((block, 2 * hidden), lambda i: (i, 0)),
        ),
        out_shape=(hbm((rows, hidden)), hbm((rows, 2 * hidden), F32)),
        compiler_params=params(16),
        name="expert_forward",
    )(x, w_gate, w_up)


def turned_columns(rank, ref_count, part, n_tp):
    if ref_count == 1:
        return [0]
    start = lambda ahead: lax.rem(rank + ahead, n_tp) * part
    half = part // 2
    starts = [start(0), start(1), start(2), start(2) + half, start(3)]
    return [pl.multiple_of(at, half) for at in starts]


def backward_kernel(rank_ref, *refs, count, n_tp):
    got_refs, refs = refs[:count], refs[count:]
    slope_ref, down_ref, gate_ref, up_ref = refs[:4]
    both_ref, up1_ref, dn1_ref, up2_ref, dn2_ref, mine_ref = refs[4:]
    width = mine_ref.shape[1]
    half = width // 2
    hidden = down_ref.shape[0]
    d_act = None
    for got_ref, at in zip(got_refs, turned_columns(rank_ref[0], count, width, n_tp)):
        columns = down_ref[:, pl.ds(at, got_ref.shape[1])]
        term = lax.dot_general(got_ref[...], columns, ROWS_ROWS, preferred_element_type=F32)
        d_act = term if d_act is None else d_act + term
    d_gate = (d_act * slope_ref[:, :hidden]).astype(BF)
    d_up = (d_act * slope_ref[:, hidden:]).astype(BF)
    both_ref[:, :hidden] = d_gate
    both_ref[:, hidden:] = d_up

    def term(ahead):
        at = pl.multiple_of(lax.rem(rank_ref[0] + ahead, n_tp) * width, width)
        both = lax.dot_general(
            d_gate, gate_ref[pl.ds(at, width), :], ROWS_ROWS, preferred_element_type=F32
        )
        both = both + lax.dot_general(
            d_up, up_ref[pl.ds(at, width), :], ROWS_ROWS, preferred_element_type=F32
        )
        return both.astype(BF)

    away = term(2)
    up1_ref[:, :half] = away[:, :half]
    dn1_ref[:, :half] = away[:, half:]
    above = term(1)
    up1_ref[:, half:] = above[:, half:]
    up2_ref[...] = above[:, :half]
    below = term(3)
    dn1_ref[:, half:] = below[:, :half]
    dn2_ref[...] = below[:, half:]
    mine_ref[...] = term(0)


def expert_backward(rank, gots, slope, w_down, w_gate, w_up, n_tp):
    rows = gots[0].shape[0]
    hidden, width = w_down.shape
    part = width // n_tp
    block = 256
    by_rows = lambda cols: pl.BlockSpec((block, cols), lambda i: (i, 0))
    whole = pl.BlockSpec(memory_space=pltpu.VMEM)
    outs = (2 * hidden, part, part, part // 2, part // 2, part)
    return pl.pallas_call(
        functools.partial(backward_kernel, count=len(gots), n_tp=n_tp),
        grid=(rows // block,),
        in_specs=[pl.BlockSpec(memory_space=pltpu.SMEM)]
        + [by_rows(g.shape[1]) for g in gots]
        + [
            by_rows(2 * hidden),
            whole,
            whole,
            whole,
        ],
        out_specs=tuple(by_rows(c) for c in outs),
        out_shape=tuple(hbm((rows, c)) for c in outs),
        compiler_params=params(16),
        name="expert_backward",
    )(rank, *gots, slope, w_down, w_gate, w_up)


def summed_products(lefts, rights):
    total = None
    for left, right in zip(lefts, rights):
        term = lax.dot_general(left[...], right[...], COLS_COLS, preferred_element_type=F32)
        total = term if total is None else total + term
    return total


def gate_up_kernel(*refs, groups):
    gate_ref, up_ref = refs[2 * groups :]
    total = summed_products(refs[:groups], refs[groups : 2 * groups])
    hidden = gate_ref.shape[1]
    gate_ref[...] = total[:, :hidden].astype(BF)
    up_ref[...] = total[:, hidden:].astype(BF)


def gate_up_grads(saved, both):
    width, hidden = saved[0].shape[1], both[0].shape[1] // 2
    block = 256
    out = pl.BlockSpec((block, hidden), lambda i: (i, 0))
    return pl.pallas_call(
        functools.partial(gate_up_kernel, groups=len(saved)),
        grid=(width // block,),
        in_specs=[pl.BlockSpec((x.shape[0], block), lambda i: (0, i)) for x in saved]
        + [pl.BlockSpec(g.shape, lambda i: (0, 0)) for g in both],
        out_specs=(out, out),
        out_shape=(jax.ShapeDtypeStruct((width, hidden), BF),) * 2,
        compiler_params=params(16),
        name="gate_up_grads",
    )(*saved, *both)


def down_kernel(rank_ref, first_act, second_act, *refs, n_tp):
    pieces, second, out_ref = refs[:-2], refs[-2], refs[-1]
    part = second.shape[1] // n_tp
    for piece, at in zip(pieces, turned_columns(rank_ref[0], len(pieces), part, n_tp)):
        columns = pl.ds(at, piece.shape[1])
        total = lax.dot_general(first_act[...], piece[...], COLS_COLS, preferred_element_type=F32)
        total = total + lax.dot_general(
            second_act[...], second[:, columns], COLS_COLS, preferred_element_type=F32
        )
        out_ref[:, columns] = total.astype(BF)


def down_grads(rank, acts, received, n_tp):
    pieces, (second,) = received
    arrays = (*acts, *pieces, second)
    whole = lambda *shape: pl.BlockSpec(shape, lambda i: (0, 0))
    out = (acts[0].shape[1], second.shape[1])
    return pl.pallas_call(
        functools.partial(down_kernel, n_tp=n_tp),
        grid=(1,),
        in_specs=[pl.BlockSpec(memory_space=pltpu.SMEM)] + [whole(*a.shape) for a in arrays],
        out_specs=whole(*out),
        out_shape=hbm(out),
        compiler_params=params(32),
        name="down_grads",
    )(rank, *in_hbm(*arrays))


def ring(n, step):
    return [(i, (i + step) % n) for i in range(n)]


def gathered_over_tp(x, n_tp):
    half = x.shape[1] // 2
    below = lax.ppermute(x, "tp", ring(n_tp, 1))
    above = lax.ppermute(x, "tp", ring(n_tp, -1))
    left, right = below[:, :half], above[:, half:]
    left = lax.ppermute(left, "tp", ring(n_tp, 1))
    right = lax.ppermute(right, "tp", ring(n_tp, -1))
    return below, above, left, right


def summed_over_tp(up1, dn1, up2, dn2, mine, n_tp):
    half = up2.shape[1]
    from_below = lax.ppermute(up1, "tp", ring(n_tp, 1))
    from_above = lax.ppermute(dn1, "tp", ring(n_tp, -1))
    add = lambda a, b: (a.astype(F32) + b.astype(F32)).astype(BF)
    up2 = add(up2, from_below[:, :half])
    dn2 = add(dn2, from_above[:, :half])
    left = lax.ppermute(up2, "tp", ring(n_tp, 1))
    right = lax.ppermute(dn2, "tp", ring(n_tp, -1))
    far = jnp.concatenate([left, right], axis=1).astype(F32)
    near = jnp.concatenate([from_above[:, half:], from_below[:, half:]], axis=1).astype(F32)
    return (mine.astype(F32) + far + near).astype(BF)


def combine_kernel(col_ref, cot_ref, back_ref, out_ref):
    tokens, top = col_ref.shape
    at = iota((tokens, back_ref.shape[0]), 1)
    hit = col_ref[:, 0:1] == at
    for k in range(1, top):
        hit = hit | (col_ref[:, k : k + 1] == at)
    total = jnp.dot(hit.astype(F32).astype(BF), back_ref[...], preferred_element_type=F32)
    out_ref[...] = (cot_ref[...].astype(F32) + total).astype(BF)


def combine(col, cot_part, back):
    return pl.pallas_call(
        combine_kernel,
        out_shape=jax.ShapeDtypeStruct(cot_part.shape, BF),
        compiler_params=params(16),
        name="combine",
    )(col, cot_part, back)


def pieces_of(rank_ref, z_refs, n_tp):
    z0, z_below, z_above, z_top, z_bottom = z_refs
    me = rank_ref[0]
    away = jnp.concatenate([z_top[...], z_bottom[...]], axis=1)
    order = ((0, z0[...]), (n_tp - 1, z_below[...]), (1, z_above[...]), (2, away))
    width = z0.shape[1]
    return [(pl.multiple_of(lax.rem(me + a, n_tp) * width, width), z) for a, z in order]


def state_kernel(
    rank_ref,
    z0,
    z1,
    z2,
    z3,
    z4,
    w_hbm,
    mixed_ref,
    branch_ref,
    decay_ref,
    later_ref,
    earlier_ref,
    branch_grad_ref,
    state_ref,
    carry_ref,
    w_ref,
    sem,
    *,
    n_tp,
):
    copy = pltpu.make_async_copy(w_hbm, w_ref, sem)
    copy.start()
    copy.wait()
    total = None
    for at, z in pieces_of(rank_ref, (z0, z1, z2, z3, z4), n_tp):
        term = jnp.dot(z, w_ref[pl.ds(at, z.shape[1]), :], preferred_element_type=F32)
        total = term if total is None else total + term
    branch_grad_ref[...] = (total * mixed_ref[...].astype(F32)).astype(BF)
    state = total * branch_ref[...].astype(F32)
    state_ref[...] = state
    scaled = state * decay_ref[...]
    ahead = jnp.sum(scaled * earlier_ref[...], axis=0, keepdims=True)
    behind = jnp.sum(scaled * later_ref[...], axis=0, keepdims=True)
    last = slice(state.shape[0] - 1, state.shape[0])
    through = decay_ref[last, :] * earlier_ref[last, :]
    lanes = carry_ref.shape[2]
    count = ahead.shape[1] // lanes
    tile = jnp.concatenate(
        [
            v[:, b * lanes : (b + 1) * lanes]
            for v in (ahead, behind, through, through)
            for b in range(count)
        ],
        axis=0,
    )
    carry_ref[...] = jnp.broadcast_to(tile[None], carry_ref.shape)


def state_grads(rank, zs, w_out, mixed, branch, decay, later_prod, earlier_prod, n_sp, n_tp):
    tokens, channels = mixed.shape
    full = lambda *shape: pl.BlockSpec(shape, lambda i: (0,) * len(shape))
    held = full(tokens, channels)
    carry = (n_sp, 16, channels // 4)
    return pl.pallas_call(
        functools.partial(state_kernel, n_tp=n_tp),
        grid=(1,),
        in_specs=[pl.BlockSpec(memory_space=pltpu.SMEM)]
        + [full(*z.shape) for z in zs]
        + [pl.BlockSpec(memory_space=pl.ANY)]
        + [held] * 5,
        out_specs=(held, held, full(*carry)),
        out_shape=(hbm((tokens, channels)), hbm((tokens, channels), F32), hbm(carry, F32)),
        scratch_shapes=[pltpu.VMEM(w_out.shape, BF), pltpu.SemaphoreType.DMA(())],
        compiler_params=params(32),
        name="state_grads",
    )(rank, *zs, *in_hbm(w_out, mixed, branch, decay, later_prod, earlier_prod))


def proj_kernel(rank_ref, core_ref, z_ref, own, above, left, right, below, keep_ref, send_ref, *, n_tp, size):
    z = z_ref[...]
    me = rank_ref[0]
    same = lax.rem(me + core_ref[0], 2) == 0

    def term(ahead):
        if ahead == 2:
            channels = jnp.concatenate([left[...], right[...]], axis=1)
        else:
            channels = {0: own, 1: above, 3: below}[ahead][...]
        return lax.dot_general(z, channels, COLS_COLS, preferred_element_type=F32).astype(BF)

    for a, b in ((0, 1), (2, 3)):
        first, second = term(a), term(b)
        at = [lax.rem(me + ahead, n_tp) // 2 for ahead in (a, b)]
        kept = jnp.where(same, at[0], at[1]) * size
        sent = jnp.where(same, at[1], at[0]) * size
        for i in range(first.shape[0] // size):
            rows = slice(i * size, (i + 1) * size)
            base = i * (n_tp // 2) * size
            keep_ref[pl.ds(pl.multiple_of(base + kept, size), size), :] = jnp.where(
                same, first[rows], second[rows]
            )
            send_ref[pl.ds(pl.multiple_of(base + sent, size), size), :] = jnp.where(
                same, second[rows], first[rows]
            )


def proj_terms(rank, core, z, gateds, n_tp, n_sp):
    features, channels = z.shape[1], gateds[0].shape[1]
    size = features * n_tp // n_sp
    half = jax.ShapeDtypeStruct((features * n_tp // 2, channels), BF)
    return pl.pallas_call(
        functools.partial(proj_kernel, n_tp=n_tp, size=size),
        in_specs=[pl.BlockSpec(memory_space=pltpu.SMEM)] * 2
        + [pl.BlockSpec(memory_space=pltpu.VMEM)] * 6,
        out_shape=(half, half),
        compiler_params=params(20),
        name="proj_terms",
    )(rank, core, z, *gateds)


def carried_in(me, got_ref):
    count, half = got_ref.shape[0], got_ref.shape[1] // 2
    carry = lambda q: got_ref[q, :half, :]
    through = lambda q: got_ref[q, half:, :]
    zero = jnp.zeros((half, got_ref.shape[2]), F32)
    ahead, behind = zero, zero
    for q in range(count):
        p = count - 1 - q
        ahead = jnp.where(p > me, carry(p) + through(p) * ahead, ahead)
        behind = jnp.where(q < me, carry(q) + through(q) * behind, behind)
    return ahead[: half // 2], behind[half // 2 :]


def final_kernel(
    me_ref,
    got_ref,
    state_ref,
    decay_ref,
    h_later,
    h_earlier,
    q_ref,
    r_ref,
    rec_w,
    inp_w,
    out_ref,
    later_ref,
    earlier_ref,
):
    rows = state_ref.shape[0]
    ahead, behind = carried_in(me_ref[0], got_ref)
    spread = lambda v: jnp.concatenate([v[b : b + 1] for b in range(v.shape[0])], axis=1)

    def step(i, carry):
        ahead, behind = carry
        t = rows - 1 - i
        later = state_ref[pl.ds(t, 1), :] + ahead
        later_ref[pl.ds(t, 1), :] = later
        earlier = state_ref[pl.ds(i, 1), :] + behind
        earlier_ref[pl.ds(i, 1), :] = earlier
        return (later * decay_ref[pl.ds(t, 1), :], earlier * decay_ref[pl.ds(i, 1), :])

    lax.fori_loop(0, rows, step, (spread(ahead), spread(behind)), unroll=8)
    later, earlier = later_ref[...], earlier_ref[...]
    total = later + earlier
    rec_pre = (later * h_later[...] + earlier * h_earlier[...]).astype(BF)
    inp_pre = (total * q_ref[...]).astype(BF)
    direct = total * r_ref[...]
    size = rec_w.shape[1]
    for b in range(rec_w.shape[0]):
        cols = slice(b * size, (b + 1) * size)
        term = lax.dot_general(rec_pre[:, cols], rec_w[b], ROWS_ROWS, preferred_element_type=F32)
        term = term + lax.dot_general(
            inp_pre[:, cols], inp_w[b], ROWS_ROWS, preferred_element_type=F32
        )
        out_ref[:, cols] = (direct[:, cols] + term).astype(BF)


def final_grads(me, got, arrays, rec_w, inp_w):
    tokens, channels = arrays[0].shape
    rows = pl.BlockSpec((tokens, channels), lambda i: (0, 0))
    fixed = lambda a: pl.BlockSpec(a.shape, lambda i: (0,) * a.ndim)
    return pl.pallas_call(
        final_kernel,
        grid=(1,),
        in_specs=[pl.BlockSpec(memory_space=pltpu.SMEM), fixed(got)]
        + [rows] * len(arrays)
        + [fixed(rec_w), fixed(inp_w)],
        out_specs=rows,
        out_shape=hbm((tokens, channels)),
        scratch_shapes=[pltpu.VMEM((tokens, channels), F32)] * 2,
        compiler_params=params(32),
        name="final_grads",
    )(me, got, *in_hbm(*arrays, rec_w, inp_w))


def blockwise(rows, weights):
    size = weights.shape[1]
    return jnp.concatenate(
        [
            jnp.dot(rows[:, b * size : (b + 1) * size], weights[b], preferred_element_type=F32)
            for b in range(weights.shape[0])
        ],
        axis=1,
    )


def shards(
    output_cotangent,
    chosen_expert_index,
    chosen_expert_weight,
    expert_slot_tokens,
    expert_gate_matrix,
    expert_up_matrix,
    expert_down_matrix,
    output_projection_matrix,
    recurrence_input,
    branch_activation_values,
    forward_scan_state,
    reverse_scan_state,
    channel_decay_rate,
    position_extra_log_decay,
    recurrence_gate_weights,
    input_gate_weights,
):
    n_sp = lax.axis_size("sp")
    n_tp = lax.axis_size("tp")
    tokens, model_width = output_cotangent.shape
    experts = n_sp * expert_gate_matrix.shape[0]
    capacity = expert_slot_tokens.shape[1] // n_sp
    slots = expert_slot_tokens.shape[1]
    part = model_width // n_tp
    rank = lax.axis_index("tp").astype(jnp.int32).reshape(1)
    place = lax.axis_index("sp").astype(jnp.int32).reshape(1)
    bounds, at = [], 0
    for size in SLOT_GROUPS:
        bounds.append((at, size))
        at += size

    col, row = slot_rows(chosen_expert_index, experts)
    weight_t = chosen_expert_weight.T
    cot_part = lax.dynamic_slice_in_dim(output_cotangent, rank[0] * part, part, 1)
    w_gate, w_up, w_down = expert_gate_matrix[0], expert_up_matrix[0], expert_down_matrix[0]
    received = []
    for g, (base, size) in enumerate(bounds):
        cot = output_cotangent if g else cot_part
        out = dispatch(row, weight_t, cot, base * experts, size * experts)
        got = lax.all_to_all(out.reshape(experts, size, -1), "sp", 0, 0, tiled=True)
        got = got.reshape(n_sp * size, -1)
        if g:
            received.append((got,))
        else:
            below, above, left, right = gathered_over_tp(got, n_tp)
            received.append((got, above, left, right, below))
    w_down, w_gate_held, w_up_held = held(w_down, w_gate, w_up)

    by_source = expert_slot_tokens.reshape(n_sp, capacity, model_width)
    saved, acts, slopes = [], [], []
    for g, (base, size) in enumerate(bounds):
        x = by_source[:, base : base + size].reshape(n_sp * size, model_width)
        if g:
            w_gate, w_up = w_gate_held, w_up_held
        act, slope = expert_forward(x, w_gate, w_up)
        saved.append(x)
        acts.append(act)
        slopes.append(slope)

    rec = jax.nn.sigmoid(blockwise(recurrence_input, recurrence_gate_weights))
    inp = jax.nn.sigmoid(blockwise(recurrence_input, input_gate_weights))
    rate = -gate_scale_factor * channel_decay_rate[None, :]
    log_decay = rec * rate + position_extra_log_decay[:, None]
    decay = jnp.exp(log_decay)
    scale_in = jnp.sqrt(-jnp.expm1(2.0 * log_decay))
    inputs = recurrence_input.astype(F32)
    xin = scale_in * inp * inputs
    mixed = (
        (decay * forward_scan_state + xin) + (decay * reverse_scan_state + xin)
    ).astype(BF)
    gated = (mixed.astype(F32) * branch_activation_values.astype(F32)).astype(BF)
    lower = (iota((tokens, tokens), 1) <= iota((tokens, tokens), 0)).astype(F32)
    running = jnp.dot(lower, log_decay, precision=lax.Precision.HIGHEST)
    later_prod = jnp.exp(running[-1:] - running)
    earlier_prod = jnp.exp(running - log_decay)
    rec_slope = rate * rec * (1.0 - rec)
    shared = inp * inputs * decay * decay / scale_in
    h_later = (forward_scan_state * decay - shared) * rec_slope
    h_earlier = (reverse_scan_state * decay - shared) * rec_slope
    q = scale_in * inputs * inp * (1.0 - inp)
    r = scale_in * inp

    boths, sums = [], []
    for g, (base, size) in enumerate(bounds):
        both, *terms = expert_backward(
            rank, received[g], slopes[g], w_down, w_gate, w_up, n_tp
        )
        sums.append(summed_over_tp(*terms, n_tp).reshape(n_sp, size, part))
        boths.append(both)
    back = lax.all_to_all(jnp.concatenate(sums, axis=1), "sp", 0, 0, tiled=True)
    gate_grad, up_grad = gate_up_grads(saved, boths)
    down_grad = down_grads(rank, acts, received, n_tp)

    below, above, left, right = gathered_over_tp(gated, n_tp)
    gateds = (gated, above, left, right, below)

    z0 = combine(col, cot_part, back.reshape(slots, part))
    zs = (z0, *gathered_over_tp(z0, n_tp))

    keep, send = proj_terms(rank, place % 2, z0, gateds, n_tp, n_sp)
    other = lax.ppermute(send, "sp", [(i, i ^ 1) for i in range(n_sp)])
    terms = (keep.astype(F32) + other.astype(F32)).astype(BF)
    terms = terms.reshape(n_sp // 2, model_width // n_sp, -1)
    groups = [list(range(c, n_sp, 2)) for c in range(2)]
    terms = lax.all_to_all(terms, "sp", 0, 0, axis_index_groups=groups, tiled=True)
    proj_grad = jnp.sum(terms.astype(F32), axis=0)
    spread = n_sp // n_tp
    moves = [
        (s * n_tp + x, (x * spread + s // n_tp) * n_tp + s % n_tp)
        for s in range(n_sp)
        for x in range(n_tp)
    ]
    proj_grad = lax.ppermute(proj_grad, ("sp", "tp"), moves)

    branch_grad, state, carry = state_grads(
        rank,
        zs,
        output_projection_matrix,
        mixed,
        branch_activation_values,
        decay,
        later_prod,
        earlier_prod,
        n_sp,
        n_tp,
    )
    carried = lax.all_to_all(carry, "sp", 0, 0, tiled=True)
    input_grad = final_grads(
        place,
        carried,
        (state, decay, h_later, h_earlier, q, r),
        recurrence_gate_weights,
        input_gate_weights,
    )
    return (gate_grad[None], up_grad[None], down_grad[None], proj_grad, branch_grad, input_grad)


def solution(mesh):
    in_specs = (
        P("sp", None),
        P("sp", None),
        P("sp", None),
        P("sp", None, None),
        P("sp", None, "tp"),
        P("sp", None, "tp"),
        P("sp", "tp", None),
        P(None, "tp"),
        P("sp", "tp"),
        P("sp", "tp"),
        P("sp", "tp"),
        P("sp", "tp"),
        P("tp"),
        P("sp"),
        P("tp", None, None),
        P("tp", None, None),
    )
    out_specs = (
        P("sp", None, "tp"),
        P("sp", None, "tp"),
        P("sp", "tp", None),
        P("sp", "tp"),
        P("sp", "tp"),
        P("sp", "tp"),
    )
    return jax.shard_map(shards, mesh=mesh, in_specs=in_specs, out_specs=out_specs, check_vma=False)
```

```python
import functools

import jax
import jax.numpy as jnp
from jax import lax
from jax.experimental import pallas as pl
from jax.experimental.pallas import tpu as pltpu
from jax.sharding import PartitionSpec as P


gate_scale_factor = 8.0
clamp_limit = 7.0
glu_alpha = 1.702

BF = jnp.bfloat16
F32 = jnp.float32

SLOT_GROUPS = (24, 16)

ROWS_ROWS = (((1,), (1,)), ((), ()))
COLS_COLS = (((0,), (0,)), ((), ()))


def params(limit_mib):
    return pltpu.CompilerParams(vmem_limit_bytes=limit_mib * 1024 * 1024)


def hbm(shape, dtype=BF):
    return pltpu.HBM(shape, dtype)


def in_hbm(*arrays):
    return tuple(pltpu.with_memory_space_constraint(a, pltpu.HBM) for a in arrays)


def iota(shape, dim):
    return lax.broadcasted_iota(jnp.int32, shape, dim)


def placed_row(expert, slot, experts):
    base, row = 0, None
    for size in SLOT_GROUPS:
        here = base * experts + expert * size + (slot - base)
        row = here if row is None else jnp.where(slot >= base, here, row)
        base += size
    return row


def slots_kernel(idx_ref, col_ref, *, experts):
    tokens, top = idx_ref.shape
    a, b = iota((tokens, tokens), 0), iota((tokens, tokens), 1)
    hot = [idx_ref[:, k : k + 1] == iota((tokens, experts), 1) for k in range(top)]
    both = sum(h.astype(F32) for h in hot).astype(BF)
    before = jnp.dot((b < a).astype(F32).astype(BF), both, preferred_element_type=F32)
    for k in range(top):
        rank = jnp.sum(jnp.where(hot[k], before, 0.0), axis=1, keepdims=True).astype(jnp.int32)
        col_ref[:, k : k + 1] = idx_ref[:, k : k + 1] * sum(SLOT_GROUPS) + rank


def slot_columns(chosen, experts):
    return pl.pallas_call(
        functools.partial(slots_kernel, experts=experts),
        out_shape=jax.ShapeDtypeStruct(chosen.shape, jnp.int32),
        compiler_params=params(8),
        name="slots",
    )(chosen)


def dispatch_kernel(idx_ref, weight_ref, cot_ref, out_ref, row_ref, *, first, experts):
    rows, tokens = out_ref.shape[0], cot_ref.shape[0]
    top = idx_ref.shape[0]

    @pl.when(pl.program_id(0) == 0)
    def _():
        a, b = iota((tokens, tokens), 0), iota((tokens, tokens), 1)
        hot = [idx_ref[k : k + 1, :] == iota((experts, tokens), 0) for k in range(top)]
        both = sum(h.astype(F32) for h in hot).astype(BF)
        before = jnp.dot(both, (a < b).astype(F32).astype(BF), preferred_element_type=F32)
        for k in range(top):
            rank = jnp.sum(jnp.where(hot[k], before, 0.0), axis=0, keepdims=True)
            row_ref[k : k + 1, :] = placed_row(
                idx_ref[k : k + 1, :], rank.astype(jnp.int32), experts
            )

    at = first + pl.program_id(0) * rows + iota((rows, tokens), 0)
    weight = jnp.zeros((rows, tokens), F32)
    for k in range(top):
        weight = jnp.where(row_ref[k : k + 1, :] == at, weight_ref[k : k + 1, :], weight)
    picked = jnp.dot((weight > 0.0).astype(F32).astype(BF), cot_ref[...], preferred_element_type=F32)
    out_ref[...] = (picked * jnp.sum(weight, axis=1, keepdims=True)).astype(BF)


def dispatch(chosen_t, weight_t, cot, first, count, experts):
    _, width = cot.shape
    block = 256
    return pl.pallas_call(
        functools.partial(dispatch_kernel, first=first, experts=experts),
        grid=(count // block,),
        in_specs=[
            pl.BlockSpec(chosen_t.shape, lambda i: (0, 0)),
            pl.BlockSpec(weight_t.shape, lambda i: (0, 0)),
            pl.BlockSpec(cot.shape, lambda i: (0, 0)),
        ],
        out_specs=pl.BlockSpec((block, width), lambda i: (i, 0)),
        out_shape=hbm((count, width)),
        scratch_shapes=[pltpu.VMEM(chosen_t.shape, jnp.int32)],
        compiler_params=params(10),
        name="dispatch",
    )(chosen_t, weight_t, cot)


def weight_copies(rank, down, gate, up, down_to, cat_to, sems, n_tp, cat_only=False):
    hidden, part = gate.shape[1], down.shape[1] // n_tp
    copies = []
    for m in range(n_tp):
        at = pl.multiple_of(lax.rem(rank + m, n_tp) * part, part)
        copies.append((down.at[:, pl.ds(at, part)], down_to.at[:, m * part : (m + 1) * part]))
    copies.append((gate, cat_to.at[:, :hidden]))
    copies.append((up, cat_to.at[:, hidden:]))
    first = n_tp if cat_only else 0
    return [
        pltpu.make_async_copy(a, b, sems.at[first + i])
        for i, (a, b) in enumerate(copies[first:])
    ]


def fetch_kernel(rank_ref, down, gate, up, down_to, cat_to, sems, *, n_tp):
    copies = weight_copies(rank_ref[0], down, gate, up, down_to, cat_to, sems, n_tp)
    for copy in copies:
        copy.start()
    for copy in copies:
        copy.wait()


def fetched_weights(rank, w_down, w_gate, w_up, n_tp):
    width, hidden = w_gate.shape
    return pl.pallas_call(
        functools.partial(fetch_kernel, n_tp=n_tp),
        in_specs=[pl.BlockSpec(memory_space=pltpu.SMEM)]
        + [pl.BlockSpec(memory_space=pl.ANY)] * 3,
        out_specs=(pl.BlockSpec(memory_space=pltpu.VMEM),) * 2,
        out_shape=(pltpu.VMEM(w_down.shape, BF), pltpu.VMEM((width, 2 * hidden), BF)),
        scratch_shapes=[pltpu.SemaphoreType.DMA((n_tp + 2,))],
        compiler_params=params(4),
        name="fetch",
    )(rank, *in_hbm(w_down, w_gate, w_up))


def forward_kernel(x_ref, *refs):
    weights, (act_ref, slope_ref) = refs[:-2], refs[-2:]
    x = x_ref[...]
    hidden = act_ref.shape[1]
    pre = [jnp.dot(x, w[...], preferred_element_type=F32) for w in weights]
    gate_pre, up_pre = pre if len(pre) == 2 else (pre[0][:, :hidden], pre[0][:, hidden:])
    glu = jnp.minimum(gate_pre, clamp_limit)
    lin = jnp.clip(up_pre, -clamp_limit, clamp_limit) + 1.0
    sig = 1.0 / (1.0 + jnp.exp(-glu_alpha * glu))
    silu = glu * sig
    act_ref[...] = (silu * lin).astype(BF)
    slope = lin * (sig + glu_alpha * silu * (1.0 - sig))
    slope_ref[:, :hidden] = jnp.where(gate_pre < clamp_limit, slope, 0.0)
    slope_ref[:, hidden:] = jnp.where(jnp.abs(up_pre) < clamp_limit, silu, 0.0)


def expert_forward(x, weights, hidden):
    rows, width = x.shape
    block = 384 if rows % 384 == 0 else 256
    whole = pl.BlockSpec(memory_space=pltpu.VMEM)
    return pl.pallas_call(
        forward_kernel,
        grid=(rows // block,),
        in_specs=[pl.BlockSpec((block, width), lambda i: (i, 0))] + [whole] * len(weights),
        out_specs=(
            pl.BlockSpec((block, hidden), lambda i: (i, 0)),
            pl.BlockSpec((block, 2 * hidden), lambda i: (i, 0)),
        ),
        out_shape=(hbm((rows, hidden)), hbm((rows, 2 * hidden), F32)),
        compiler_params=params(24),
        name="expert_forward",
    )(x, *weights)


def backward_kernel(rank_ref, *refs, count, fetched, n_tp):
    got_refs, refs = refs[:count], refs[count:]
    slope_ref, refs = refs[0], refs[1:]
    sources, refs = (refs[:3], refs[3:]) if fetched else ((), refs)
    weights, refs = ((), refs) if fetched else (refs[:2], refs[2:])
    both_ref, up1_ref, dn1_ref, up2_ref, dn2_ref, mine_ref = refs[:6]
    first = pl.program_id(0) == 0
    if fetched:
        weights, sems = refs[6:8], refs[8]

        @pl.when(first)
        def _():
            copies = weight_copies(0, *sources, *weights, sems, n_tp)
            for copy in copies:
                copy.start()
            for copy in copies[:n_tp]:
                copy.wait()

    down_ref, cat_ref = weights
    width = mine_ref.shape[1]
    half = width // 2
    hidden = down_ref.shape[0]
    got = [ref[...] for ref in got_refs]
    got = got[0] if len(got) == 1 else jnp.concatenate(got, axis=1)
    d_act = lax.dot_general(got, down_ref[...], ROWS_ROWS, preferred_element_type=F32)
    both_ref[:, :hidden] = (d_act * slope_ref[:, :hidden]).astype(BF)
    both_ref[:, hidden:] = (d_act * slope_ref[:, hidden:]).astype(BF)
    if fetched:

        @pl.when(first)
        def _():
            for copy in weight_copies(0, *sources, *weights, sems, n_tp, True):
                copy.wait()

    both = both_ref[...]

    def term(ahead):
        at = pl.multiple_of(lax.rem(rank_ref[0] + ahead, n_tp) * width, width)
        return lax.dot_general(
            both, cat_ref[pl.ds(at, width), :], ROWS_ROWS, preferred_element_type=F32
        ).astype(BF)

    away = term(2)
    up1_ref[:, :half] = away[:, :half]
    dn1_ref[:, :half] = away[:, half:]
    above = term(1)
    up1_ref[:, half:] = above[:, half:]
    up2_ref[...] = above[:, :half]
    below = term(3)
    dn1_ref[:, half:] = below[:, :half]
    dn2_ref[...] = below[:, half:]
    mine_ref[...] = term(0)


def expert_backward(rank, gots, slope, weights, n_tp):
    rows = gots[0].shape[0]
    hidden, width = weights[0].shape
    part = width // n_tp
    fetched = len(weights) == 3
    block = 384 if rows % 384 == 0 and not fetched else 256
    by_rows = lambda cols: pl.BlockSpec((block, cols), lambda i: (i, 0))
    whole = pl.BlockSpec(memory_space=pl.ANY if fetched else pltpu.VMEM)
    scratch = [
        pltpu.VMEM((hidden, width), BF),
        pltpu.VMEM((width, 2 * hidden), BF),
        pltpu.SemaphoreType.DMA((n_tp + 2,)),
    ]
    if fetched:
        slope, *weights = in_hbm(slope, *weights)
    outs = (2 * hidden, part, part, part // 2, part // 2, part)
    return pl.pallas_call(
        functools.partial(backward_kernel, count=len(gots), fetched=fetched, n_tp=n_tp),
        grid=(rows // block,),
        in_specs=[pl.BlockSpec(memory_space=pltpu.SMEM)]
        + [by_rows(g.shape[1]) for g in gots]
        + [by_rows(2 * hidden)]
        + [whole] * len(weights),
        out_specs=tuple(by_rows(c) for c in outs),
        out_shape=tuple(hbm((rows, c)) for c in outs),
        scratch_shapes=scratch if fetched else [],
        compiler_params=params(24),
        name="expert_backward",
    )(rank, *gots, slope, *weights)


def summed_products(lefts, rights):
    total = None
    for left, right in zip(lefts, rights):
        term = lax.dot_general(left[...], right[...], COLS_COLS, preferred_element_type=F32)
        total = term if total is None else total + term
    return total


def gate_up_kernel(*refs, groups):
    gate_ref, up_ref = refs[2 * groups :]
    total = summed_products(refs[:groups], refs[groups : 2 * groups])
    hidden = gate_ref.shape[1]
    gate_ref[...] = total[:, :hidden].astype(BF)
    up_ref[...] = total[:, hidden:].astype(BF)


def gate_up_grads(saved, both):
    width, hidden = saved[0].shape[1], both[0].shape[1] // 2
    block = 512
    out = pl.BlockSpec((block, hidden), lambda i: (i, 0))
    return pl.pallas_call(
        functools.partial(gate_up_kernel, groups=len(saved)),
        grid=(width // block,),
        in_specs=[pl.BlockSpec((x.shape[0], block), lambda i: (0, i)) for x in saved]
        + [pl.BlockSpec(g.shape, lambda i: (0, 0)) for g in both],
        out_specs=(out, out),
        out_shape=(jax.ShapeDtypeStruct((width, hidden), BF),) * 2,
        compiler_params=params(32),
        name="gate_up_grads",
    )(*in_hbm(*saved, *both))


def down_kernel(rank_ref, first_act, second_act, second, *refs, count, n_tp):
    pieces, refs = refs[:count], refs[count:]
    out_ref, act0, act1, rows0, rows1, turned0, turned1, sems = refs
    part = second.shape[1] // n_tp
    half = part // 2
    pairs = [(first_act, act0), (second_act, act1), (second, rows1)]
    for i, piece in enumerate(pieces):
        ahead, side = (0, 0) if i == 0 else ((i + 1) // 2, (i + 1) % 2)
        at = lax.rem(rank_ref[0] + ahead, n_tp) * part + side * half
        columns = pl.ds(pl.multiple_of(at, half), piece.shape[1])
        pairs.append((piece, rows0.at[:, columns]))
    copies = [pltpu.make_async_copy(a, b, sems.at[i]) for i, (a, b) in enumerate(pairs)]
    for copy in copies:
        copy.start()
    for copy in copies[:2]:
        copy.wait()
    turned0[...] = act0[...].T
    turned1[...] = act1[...].T
    for copy in copies[2:]:
        copy.wait()
    for m in range(n_tp):
        columns = slice(m * part, (m + 1) * part)
        total = jnp.dot(turned0[...], rows0[:, columns], preferred_element_type=F32)
        total = total + jnp.dot(turned1[...], rows1[:, columns], preferred_element_type=F32)
        out_ref[:, columns] = total.astype(BF)


def down_grads(rank, acts, received, n_tp):
    pieces, (second,) = received
    arrays = (*acts, second, *pieces)
    hidden, width = acts[0].shape[1], second.shape[1]
    counts = [a.shape[0] for a in acts]
    return pl.pallas_call(
        functools.partial(down_kernel, count=len(pieces), n_tp=n_tp),
        grid=(1,),
        in_specs=[pl.BlockSpec(memory_space=pltpu.SMEM)]
        + [pl.BlockSpec(memory_space=pl.ANY)] * len(arrays),
        out_specs=pl.BlockSpec((hidden, width), lambda i: (0, 0)),
        out_shape=hbm((hidden, width)),
        scratch_shapes=[pltpu.VMEM((n, hidden), BF) for n in counts]
        + [pltpu.VMEM((n, width), BF) for n in counts]
        + [pltpu.VMEM((hidden, n), BF) for n in counts]
        + [pltpu.SemaphoreType.DMA((len(arrays),))],
        compiler_params=params(32),
        name="down_grads",
    )(rank, *in_hbm(*arrays))


def ring(n, step):
    return [(i, (i + step) % n) for i in range(n)]


def gathered_over_tp(x, n_tp):
    half = x.shape[1] // 2
    below = lax.ppermute(x, "tp", ring(n_tp, 1))
    above = lax.ppermute(x, "tp", ring(n_tp, -1))
    left, right = below[:, :half], above[:, half:]
    left = lax.ppermute(left, "tp", ring(n_tp, 1))
    right = lax.ppermute(right, "tp", ring(n_tp, -1))
    return below, above, left, right


def gathered_early(x, n_tp):
    half = x.shape[1] // 2
    left, right = x[:, :half], x[:, half:]
    up, down = ring(n_tp, 1), ring(n_tp, -1)
    below_left = lax.ppermute(left, "tp", up)
    above_right = lax.ppermute(right, "tp", down)
    below_right = lax.ppermute(right, "tp", up)
    above_left = lax.ppermute(left, "tp", down)
    away_left = lax.ppermute(below_left, "tp", up)
    away_right = lax.ppermute(above_right, "tp", down)
    return (x, above_left, above_right, away_left, away_right, below_left, below_right)


def summed_over_tp(up1, dn1, up2, dn2, mine, n_tp):
    half = up2.shape[1]
    from_below = lax.ppermute(up1, "tp", ring(n_tp, 1))
    from_above = lax.ppermute(dn1, "tp", ring(n_tp, -1))
    add = lambda a, b: (a.astype(F32) + b.astype(F32)).astype(BF)
    up2 = add(up2, from_below[:, :half])
    dn2 = add(dn2, from_above[:, :half])
    left = lax.ppermute(up2, "tp", ring(n_tp, 1))
    right = lax.ppermute(dn2, "tp", ring(n_tp, -1))
    far = jnp.concatenate([left, right], axis=1).astype(F32)
    near = jnp.concatenate([from_above[:, half:], from_below[:, half:]], axis=1).astype(F32)
    return (mine.astype(F32) + far + near).astype(BF)


def combine_kernel(col_ref, cot_ref, back_ref, out_ref):
    tokens, top = col_ref.shape
    at = iota((tokens, back_ref.shape[0]), 1)
    hit = col_ref[:, 0:1] == at
    for k in range(1, top):
        hit = hit | (col_ref[:, k : k + 1] == at)
    total = jnp.dot(hit.astype(F32).astype(BF), back_ref[...], preferred_element_type=F32)
    out_ref[...] = (cot_ref[...].astype(F32) + total).astype(BF)


def combine(col, cot_part, back):
    return pl.pallas_call(
        combine_kernel,
        out_shape=jax.ShapeDtypeStruct(cot_part.shape, BF),
        compiler_params=params(16),
        name="combine",
    )(col, cot_part, back)


def pieces_of(rank_ref, z_refs, n_tp):
    z0, z_below, z_above, z_top, z_bottom = z_refs
    me = rank_ref[0]
    away = jnp.concatenate([z_top[...], z_bottom[...]], axis=1)
    order = ((0, z0[...]), (n_tp - 1, z_below[...]), (1, z_above[...]), (2, away))
    width = z0.shape[1]
    return [(pl.multiple_of(lax.rem(me + a, n_tp) * width, width), z) for a, z in order]


def state_kernel(
    rank_ref,
    z0,
    z1,
    z2,
    z3,
    z4,
    w_hbm,
    mixed_ref,
    branch_ref,
    decay_ref,
    later_ref,
    earlier_ref,
    branch_grad_ref,
    state_ref,
    carry_ref,
    w_ref,
    sem,
    *,
    n_tp,
):
    copy = pltpu.make_async_copy(w_hbm, w_ref, sem)
    copy.start()
    copy.wait()
    total = None
    for at, z in pieces_of(rank_ref, (z0, z1, z2, z3, z4), n_tp):
        term = jnp.dot(z, w_ref[pl.ds(at, z.shape[1]), :], preferred_element_type=F32)
        total = term if total is None else total + term
    branch_grad_ref[...] = (total * mixed_ref[...].astype(F32)).astype(BF)
    state = total * branch_ref[...].astype(F32)
    state_ref[...] = state
    scaled = state * decay_ref[...]
    ahead = jnp.sum(scaled * earlier_ref[...], axis=0, keepdims=True)
    behind = jnp.sum(scaled * later_ref[...], axis=0, keepdims=True)
    last = slice(state.shape[0] - 1, state.shape[0])
    through = decay_ref[last, :] * earlier_ref[last, :]
    lanes = carry_ref.shape[2]
    count = ahead.shape[1] // lanes
    tile = jnp.concatenate(
        [
            v[:, b * lanes : (b + 1) * lanes]
            for v in (ahead, behind, through, through)
            for b in range(count)
        ],
        axis=0,
    )
    carry_ref[...] = jnp.broadcast_to(tile[None], carry_ref.shape)


def state_grads(rank, zs, w_out, mixed, branch, decay, later_prod, earlier_prod, n_sp, n_tp):
    tokens, channels = mixed.shape
    full = lambda *shape: pl.BlockSpec(shape, lambda i: (0,) * len(shape))
    held = full(tokens, channels)
    carry = (n_sp, 16, channels // 4)
    return pl.pallas_call(
        functools.partial(state_kernel, n_tp=n_tp),
        grid=(1,),
        in_specs=[pl.BlockSpec(memory_space=pltpu.SMEM)]
        + [full(*z.shape) for z in zs]
        + [pl.BlockSpec(memory_space=pl.ANY)]
        + [held] * 5,
        out_specs=(held, held, full(*carry)),
        out_shape=(hbm((tokens, channels)), hbm((tokens, channels), F32), hbm(carry, F32)),
        scratch_shapes=[pltpu.VMEM(w_out.shape, BF), pltpu.SemaphoreType.DMA(())],
        compiler_params=params(32),
        name="state_grads",
    )(rank, *zs, *in_hbm(w_out, mixed, branch, decay, later_prod, earlier_prod))


def proj_kernel(rank_ref, core_ref, z_ref, own, above, left, right, below, keep_ref, send_ref, *, n_tp, size):
    z = z_ref[...]
    me = rank_ref[0]
    same = lax.rem(me + core_ref[0], 2) == 0

    def term(ahead):
        if ahead == 2:
            channels = jnp.concatenate([left[...], right[...]], axis=1)
        else:
            channels = {0: own, 1: above, 3: below}[ahead][...]
        return lax.dot_general(z, channels, COLS_COLS, preferred_element_type=F32).astype(BF)

    for a, b in ((0, 1), (2, 3)):
        first, second = term(a), term(b)
        at = [lax.rem(me + ahead, n_tp) // 2 for ahead in (a, b)]
        kept = jnp.where(same, at[0], at[1]) * size
        sent = jnp.where(same, at[1], at[0]) * size
        for i in range(first.shape[0] // size):
            rows = slice(i * size, (i + 1) * size)
            base = i * (n_tp // 2) * size
            keep_ref[pl.ds(pl.multiple_of(base + kept, size), size), :] = jnp.where(
                same, first[rows], second[rows]
            )
            send_ref[pl.ds(pl.multiple_of(base + sent, size), size), :] = jnp.where(
                same, second[rows], first[rows]
            )


def proj_terms(rank, core, z, gateds, n_tp, n_sp):
    features, channels = z.shape[1], gateds[0].shape[1]
    size = features * n_tp // n_sp
    half = jax.ShapeDtypeStruct((features * n_tp // 2, channels), BF)
    return pl.pallas_call(
        functools.partial(proj_kernel, n_tp=n_tp, size=size),
        in_specs=[pl.BlockSpec(memory_space=pltpu.SMEM)] * 2
        + [pl.BlockSpec(memory_space=pltpu.VMEM)] * 6,
        out_shape=(half, half),
        compiler_params=params(20),
        name="proj_terms",
    )(rank, core, z, *gateds)


def carried_in(me, got_ref):
    count, half = got_ref.shape[0], got_ref.shape[1] // 2
    carry = lambda q: got_ref[q, :half, :]
    through = lambda q: got_ref[q, half:, :]
    zero = jnp.zeros((half, got_ref.shape[2]), F32)
    ahead, behind = zero, zero
    for q in range(count):
        p = count - 1 - q
        ahead = jnp.where(p > me, carry(p) + through(p) * ahead, ahead)
        behind = jnp.where(q < me, carry(q) + through(q) * behind, behind)
    return ahead[: half // 2], behind[half // 2 :]


def final_kernel(me_ref, got_ref, *refs):
    sources, out_ref = refs[:8], refs[8]
    later_ref, earlier_ref = refs[9:11]
    holds, sems = refs[11:19], refs[19]
    copies = [pltpu.make_async_copy(a, b, sems.at[i]) for i, (a, b) in enumerate(zip(sources, holds))]
    for copy in copies:
        copy.start()
    for copy in copies[:2]:
        copy.wait()
    state_ref, decay_ref, h_later, h_earlier, q_ref, r_ref, rec_w, inp_w = holds
    rows = state_ref.shape[0]
    ahead, behind = carried_in(me_ref[0], got_ref)
    spread = lambda v: jnp.concatenate([v[b : b + 1] for b in range(v.shape[0])], axis=1)

    def step(i, carry):
        ahead, behind = carry
        t = rows - 1 - i
        later = state_ref[pl.ds(t, 1), :] + ahead
        later_ref[pl.ds(t, 1), :] = later
        earlier = state_ref[pl.ds(i, 1), :] + behind
        earlier_ref[pl.ds(i, 1), :] = earlier
        return (later * decay_ref[pl.ds(t, 1), :], earlier * decay_ref[pl.ds(i, 1), :])

    lax.fori_loop(0, rows, step, (spread(ahead), spread(behind)), unroll=8)
    for copy in copies[2:]:
        copy.wait()
    later, earlier = later_ref[...], earlier_ref[...]
    total = later + earlier
    rec_pre = (later * h_later[...] + earlier * h_earlier[...]).astype(BF)
    inp_pre = (total * q_ref[...]).astype(BF)
    direct = total * r_ref[...]
    size = rec_w.shape[1]
    for b in range(rec_w.shape[0]):
        cols = slice(b * size, (b + 1) * size)
        term = lax.dot_general(rec_pre[:, cols], rec_w[b], ROWS_ROWS, preferred_element_type=F32)
        term = term + lax.dot_general(
            inp_pre[:, cols], inp_w[b], ROWS_ROWS, preferred_element_type=F32
        )
        out_ref[:, cols] = (direct[:, cols] + term).astype(BF)


def final_grads(me, got, arrays, rec_w, inp_w):
    tokens, channels = arrays[0].shape
    sources = (*arrays, rec_w, inp_w)
    return pl.pallas_call(
        final_kernel,
        grid=(1,),
        in_specs=[
            pl.BlockSpec(memory_space=pltpu.SMEM),
            pl.BlockSpec(got.shape, lambda i: (0, 0, 0)),
        ]
        + [pl.BlockSpec(memory_space=pl.ANY)] * len(sources),
        out_specs=pl.BlockSpec((tokens, channels), lambda i: (0, 0)),
        out_shape=hbm((tokens, channels)),
        scratch_shapes=[pltpu.VMEM((tokens, channels), F32)] * 2
        + [pltpu.VMEM(a.shape, a.dtype) for a in sources]
        + [pltpu.SemaphoreType.DMA((len(sources),))],
        compiler_params=params(24),
        name="final_grads",
    )(me, got, *in_hbm(*sources))


def blockwise(rows, weights):
    size = weights.shape[1]
    return jnp.concatenate(
        [
            jnp.dot(rows[:, b * size : (b + 1) * size], weights[b], preferred_element_type=F32)
            for b in range(weights.shape[0])
        ],
        axis=1,
    )


def shards(
    output_cotangent,
    chosen_expert_index,
    chosen_expert_weight,
    expert_slot_tokens,
    expert_gate_matrix,
    expert_up_matrix,
    expert_down_matrix,
    output_projection_matrix,
    recurrence_input,
    branch_activation_values,
    forward_scan_state,
    reverse_scan_state,
    channel_decay_rate,
    position_extra_log_decay,
    recurrence_gate_weights,
    input_gate_weights,
):
    n_sp = lax.axis_size("sp")
    n_tp = lax.axis_size("tp")
    tokens, model_width = output_cotangent.shape
    experts = n_sp * expert_gate_matrix.shape[0]
    capacity = expert_slot_tokens.shape[1] // n_sp
    slots = expert_slot_tokens.shape[1]
    hidden = expert_gate_matrix.shape[2]
    part = model_width // n_tp
    rank = lax.axis_index("tp").astype(jnp.int32).reshape(1)
    place = lax.axis_index("sp").astype(jnp.int32).reshape(1)
    bounds, at = [], 0
    for size in SLOT_GROUPS:
        bounds.append((at, size))
        at += size

    chosen_t, weight_t = chosen_expert_index.T, chosen_expert_weight.T
    cot_part = lax.dynamic_slice_in_dim(output_cotangent, rank[0] * part, part, 1)
    w_gate, w_up, w_down = expert_gate_matrix[0], expert_up_matrix[0], expert_down_matrix[0]
    received = []
    for g, (base, size) in enumerate(bounds):
        cot = output_cotangent if g else cot_part
        out = dispatch(chosen_t, weight_t, cot, base * experts, size * experts, experts)
        got = lax.all_to_all(out.reshape(experts, size, -1), "sp", 0, 0, tiled=True)
        got = got.reshape(n_sp * size, -1)
        if g:
            received.append((got,))
        else:
            received.append(gathered_early(got, n_tp))
    down_turned, w_cat = fetched_weights(rank, w_down, w_gate, w_up, n_tp)

    by_source = expert_slot_tokens.reshape(n_sp, capacity, model_width)
    saved, acts, slopes = [], [], []
    for g, (base, size) in enumerate(bounds):
        x = by_source[:, base : base + size].reshape(n_sp * size, model_width)
        act, slope = expert_forward(x, (w_cat,) if g else (w_gate, w_up), hidden)
        saved.append(x)
        acts.append(act)
        slopes.append(slope)

    rec = jax.nn.sigmoid(blockwise(recurrence_input, recurrence_gate_weights))
    inp = jax.nn.sigmoid(blockwise(recurrence_input, input_gate_weights))
    rate = -gate_scale_factor * channel_decay_rate[None, :]
    log_decay = rec * rate + position_extra_log_decay[:, None]
    decay = jnp.exp(log_decay)
    scale_in = jnp.sqrt(-jnp.expm1(2.0 * log_decay))
    inputs = recurrence_input.astype(F32)
    xin = scale_in * inp * inputs
    mixed = (
        (decay * forward_scan_state + xin) + (decay * reverse_scan_state + xin)
    ).astype(BF)
    gated = (mixed.astype(F32) * branch_activation_values.astype(F32)).astype(BF)
    lower = (iota((tokens, tokens), 1) <= iota((tokens, tokens), 0)).astype(F32)
    running = jnp.dot(lower, log_decay, precision=lax.Precision.HIGHEST)
    later_prod = jnp.exp(running[-1:] - running)
    earlier_prod = jnp.exp(running - log_decay)
    rec_slope = rate * rec * (1.0 - rec)
    shared = inp * inputs * decay * decay / scale_in
    h_later = (forward_scan_state * decay - shared) * rec_slope
    h_earlier = (reverse_scan_state * decay - shared) * rec_slope
    q = scale_in * inputs * inp * (1.0 - inp)
    r = scale_in * inp

    boths, sums = [], []
    for g, (base, size) in enumerate(bounds):
        weights = (w_down, w_gate, w_up) if g else (down_turned, w_cat)
        both, *terms = expert_backward(rank, received[g], slopes[g], weights, n_tp)
        sums.append(summed_over_tp(*terms, n_tp).reshape(n_sp, size, part))
        boths.append(both)
    back = lax.all_to_all(jnp.concatenate(sums, axis=1), "sp", 0, 0, tiled=True)
    gate_grad, up_grad = gate_up_grads(saved, boths)
    down_grad = down_grads(rank, acts, received, n_tp)

    below, above, left, right = gathered_over_tp(gated, n_tp)
    gateds = (gated, above, left, right, below)

    col = slot_columns(chosen_expert_index, experts)
    z0 = combine(col, cot_part, back.reshape(slots, part))
    zs = (z0, *gathered_over_tp(z0, n_tp))

    keep, send = proj_terms(rank, place % 2, z0, gateds, n_tp, n_sp)
    other = lax.ppermute(send, "sp", [(i, i ^ 1) for i in range(n_sp)])
    terms = (keep.astype(F32) + other.astype(F32)).astype(BF)
    terms = terms.reshape(n_sp // 2, model_width // n_sp, -1)
    groups = [list(range(c, n_sp, 2)) for c in range(2)]
    terms = lax.all_to_all(terms, "sp", 0, 0, axis_index_groups=groups, tiled=True)
    proj_grad = jnp.sum(terms.astype(F32), axis=0)
    spread = n_sp // n_tp
    moves = [
        (s * n_tp + x, (x * spread + s // n_tp) * n_tp + s % n_tp)
        for s in range(n_sp)
        for x in range(n_tp)
    ]
    proj_grad = lax.ppermute(proj_grad, ("sp", "tp"), moves)

    branch_grad, state, carry = state_grads(
        rank,
        zs,
        output_projection_matrix,
        mixed,
        branch_activation_values,
        decay,
        later_prod,
        earlier_prod,
        n_sp,
        n_tp,
    )
    carried = lax.all_to_all(carry, "sp", 0, 0, tiled=True)
    input_grad = final_grads(
        place,
        carried,
        (state, decay, h_later, h_earlier, q, r),
        recurrence_gate_weights,
        input_gate_weights,
    )
    return (gate_grad[None], up_grad[None], down_grad[None], proj_grad, branch_grad, input_grad)


def solution(mesh):
    in_specs = (
        P("sp", None),
        P("sp", None),
        P("sp", None),
        P("sp", None, None),
        P("sp", None, "tp"),
        P("sp", None, "tp"),
        P("sp", "tp", None),
        P(None, "tp"),
        P("sp", "tp"),
        P("sp", "tp"),
        P("sp", "tp"),
        P("sp", "tp"),
        P("tp"),
        P("sp"),
        P("tp", None, None),
        P("tp", None, None),
    )
    out_specs = (
        P("sp", None, "tp"),
        P("sp", None, "tp"),
        P("sp", "tp", None),
        P("sp", "tp"),
        P("sp", "tp"),
        P("sp", "tp"),
    )
    return jax.shard_map(shards, mesh=mesh, in_specs=in_specs, out_specs=out_specs, check_vma=False)
```

```python
import functools

import jax
import jax.numpy as jnp
from jax import lax
from jax.experimental import pallas as pl
from jax.experimental.pallas import tpu as pltpu
from jax.sharding import PartitionSpec as P


gate_scale_factor = 8.0
clamp_limit = 7.0
glu_alpha = 1.702

BF = jnp.bfloat16
F32 = jnp.float32

SLOT_GROUPS = (24, 16)

ROWS_ROWS = (((1,), (1,)), ((), ()))
COLS_COLS = (((0,), (0,)), ((), ()))


def params(limit_mib):
    return pltpu.CompilerParams(vmem_limit_bytes=limit_mib * 1024 * 1024)


def hbm(shape, dtype=BF):
    return pltpu.HBM(shape, dtype)


def in_hbm(*arrays):
    return tuple(pltpu.with_memory_space_constraint(a, pltpu.HBM) for a in arrays)


def iota(shape, dim):
    return lax.broadcasted_iota(jnp.int32, shape, dim)


def placed_row(expert, slot, experts):
    base, row = 0, None
    for size in SLOT_GROUPS:
        here = base * experts + expert * size + (slot - base)
        row = here if row is None else jnp.where(slot >= base, here, row)
        base += size
    return row


def slots_kernel(idx_ref, col_ref, *, experts):
    tokens, top = idx_ref.shape
    a, b = iota((tokens, tokens), 0), iota((tokens, tokens), 1)
    hot = [idx_ref[:, k : k + 1] == iota((tokens, experts), 1) for k in range(top)]
    both = sum(h.astype(F32) for h in hot).astype(BF)
    before = jnp.dot((b < a).astype(F32).astype(BF), both, preferred_element_type=F32)
    for k in range(top):
        rank = jnp.sum(jnp.where(hot[k], before, 0.0), axis=1, keepdims=True).astype(jnp.int32)
        col_ref[:, k : k + 1] = idx_ref[:, k : k + 1] * sum(SLOT_GROUPS) + rank


def slot_columns(chosen, experts):
    return pl.pallas_call(
        functools.partial(slots_kernel, experts=experts),
        out_shape=jax.ShapeDtypeStruct(chosen.shape, jnp.int32),
        compiler_params=params(8),
        name="slots",
    )(chosen)


def dispatch_kernel(_, idx_ref, weight_ref, cot_ref, out_ref, row_ref, *, first, experts):
    rows, tokens = out_ref.shape[0], cot_ref.shape[0]
    top = idx_ref.shape[0]

    @pl.when(pl.program_id(0) == 0)
    def _():
        a, b = iota((tokens, tokens), 0), iota((tokens, tokens), 1)
        hot = [idx_ref[k : k + 1, :] == iota((experts, tokens), 0) for k in range(top)]
        both = sum(h.astype(F32) for h in hot).astype(BF)
        before = jnp.dot(both, (a < b).astype(F32).astype(BF), preferred_element_type=F32)
        for k in range(top):
            rank = jnp.sum(jnp.where(hot[k], before, 0.0), axis=0, keepdims=True)
            row_ref[k : k + 1, :] = placed_row(
                idx_ref[k : k + 1, :], rank.astype(jnp.int32), experts
            )

    at = first + pl.program_id(0) * rows + iota((rows, tokens), 0)
    weight = jnp.zeros((rows, tokens), F32)
    for k in range(top):
        weight = jnp.where(row_ref[k : k + 1, :] == at, weight_ref[k : k + 1, :], weight)
    picked = jnp.dot((weight > 0.0).astype(F32).astype(BF), cot_ref[...], preferred_element_type=F32)
    out_ref[...] = (picked * jnp.sum(weight, axis=1, keepdims=True)).astype(BF)


def dispatch(column, chosen_t, weight_t, cot, width, first, count, experts):
    block = 256
    return pl.pallas_call(
        functools.partial(dispatch_kernel, first=first, experts=experts),
        grid_spec=pltpu.PrefetchScalarGridSpec(
            num_scalar_prefetch=1,
            grid=(count // block,),
            in_specs=[
                pl.BlockSpec(chosen_t.shape, lambda i, c: (0, 0)),
                pl.BlockSpec(weight_t.shape, lambda i, c: (0, 0)),
                pl.BlockSpec((cot.shape[0], width), lambda i, c: (0, c[0])),
            ],
            out_specs=pl.BlockSpec((block, width), lambda i, c: (i, 0)),
            scratch_shapes=[pltpu.VMEM(chosen_t.shape, jnp.int32)],
        ),
        out_shape=hbm((count, width)),
        compiler_params=params(12),
        name="dispatch",
    )(column, chosen_t, weight_t, cot)


def weight_copies(rank, down, gate, up, down_to, cat_to, sems, n_tp, cat_only=False):
    hidden, part = gate.shape[1], down.shape[1] // n_tp
    copies = []
    for m in range(n_tp):
        at = pl.multiple_of(lax.rem(rank + m, n_tp) * part, part)
        copies.append((down.at[:, pl.ds(at, part)], down_to.at[:, m * part : (m + 1) * part]))
    copies.append((gate, cat_to.at[:, :hidden]))
    copies.append((up, cat_to.at[:, hidden:]))
    first = n_tp if cat_only else 0
    return [
        pltpu.make_async_copy(a, b, sems.at[first + i])
        for i, (a, b) in enumerate(copies[first:])
    ]


def fetch_kernel(rank_ref, down, gate, up, down_to, cat_to, sems, *, n_tp):
    copies = weight_copies(rank_ref[0], down, gate, up, down_to, cat_to, sems, n_tp)
    for copy in copies:
        copy.start()
    for copy in copies:
        copy.wait()


def fetched_weights(rank, w_down, w_gate, w_up, n_tp):
    width, hidden = w_gate.shape
    return pl.pallas_call(
        functools.partial(fetch_kernel, n_tp=n_tp),
        in_specs=[pl.BlockSpec(memory_space=pltpu.SMEM)]
        + [pl.BlockSpec(memory_space=pl.ANY)] * 3,
        out_specs=(pl.BlockSpec(memory_space=pltpu.VMEM),) * 2,
        out_shape=(pltpu.VMEM(w_down.shape, BF), pltpu.VMEM((width, 2 * hidden), BF)),
        scratch_shapes=[pltpu.SemaphoreType.DMA((n_tp + 2,))],
        compiler_params=params(4),
        name="fetch",
    )(rank, *in_hbm(w_down, w_gate, w_up))


def forward_kernel(x_ref, *refs):
    weights, (act_ref, slope_ref) = refs[:-2], refs[-2:]
    x = x_ref[...]
    hidden = act_ref.shape[1]
    pre = [jnp.dot(x, w[...], preferred_element_type=F32) for w in weights]
    gate_pre, up_pre = pre if len(pre) == 2 else (pre[0][:, :hidden], pre[0][:, hidden:])
    glu = jnp.minimum(gate_pre, clamp_limit)
    lin = jnp.clip(up_pre, -clamp_limit, clamp_limit) + 1.0
    sig = 1.0 / (1.0 + jnp.exp(-glu_alpha * glu))
    silu = glu * sig
    act_ref[...] = (silu * lin).astype(BF)
    slope = lin * (sig + glu_alpha * silu * (1.0 - sig))
    slope_ref[:, :hidden] = jnp.where(gate_pre < clamp_limit, slope, 0.0)
    slope_ref[:, hidden:] = jnp.where(jnp.abs(up_pre) < clamp_limit, silu, 0.0)


def expert_forward(x, weights, hidden):
    rows, width = x.shape
    block = 384 if rows % 384 == 0 else 256
    whole = pl.BlockSpec(memory_space=pltpu.VMEM)
    return pl.pallas_call(
        forward_kernel,
        grid=(rows // block,),
        in_specs=[pl.BlockSpec((block, width), lambda i: (i, 0))] + [whole] * len(weights),
        out_specs=(
            pl.BlockSpec((block, hidden), lambda i: (i, 0)),
            pl.BlockSpec((block, 2 * hidden), lambda i: (i, 0)),
        ),
        out_shape=(hbm((rows, hidden)), hbm((rows, 2 * hidden), F32)),
        compiler_params=params(24),
        name="expert_forward",
    )(x, *weights)


def backward_kernel(rank_ref, *refs, count, fetched, n_tp):
    got_refs, refs = refs[:count], refs[count:]
    slope_ref, refs = refs[0], refs[1:]
    sources, refs = (refs[:3], refs[3:]) if fetched else ((), refs)
    weights, refs = ((), refs) if fetched else (refs[:2], refs[2:])
    both_ref, up1_ref, dn1_ref, up2_ref, dn2_ref, mine_ref = refs[:6]
    first = pl.program_id(0) == 0
    if fetched:
        weights, sems = refs[6:8], refs[8]

        @pl.when(first)
        def _():
            copies = weight_copies(0, *sources, *weights, sems, n_tp)
            for copy in copies:
                copy.start()
            for copy in copies[:n_tp]:
                copy.wait()

    down_ref, cat_ref = weights
    width = mine_ref.shape[1]
    half = width // 2
    hidden = down_ref.shape[0]
    got = [ref[...] for ref in got_refs]
    got = got[0] if len(got) == 1 else jnp.concatenate(got, axis=1)
    d_act = lax.dot_general(got, down_ref[...], ROWS_ROWS, preferred_element_type=F32)
    both_ref[:, :hidden] = (d_act * slope_ref[:, :hidden]).astype(BF)
    both_ref[:, hidden:] = (d_act * slope_ref[:, hidden:]).astype(BF)
    if fetched:

        @pl.when(first)
        def _():
            for copy in weight_copies(0, *sources, *weights, sems, n_tp, True):
                copy.wait()

    both = both_ref[...]

    def term(ahead):
        at = pl.multiple_of(lax.rem(rank_ref[0] + ahead, n_tp) * width, width)
        return lax.dot_general(
            both, cat_ref[pl.ds(at, width), :], ROWS_ROWS, preferred_element_type=F32
        ).astype(BF)

    away = term(2)
    up1_ref[:, :half] = away[:, :half]
    dn1_ref[:, :half] = away[:, half:]
    above = term(1)
    up1_ref[:, half:] = above[:, half:]
    up2_ref[...] = above[:, :half]
    below = term(3)
    dn1_ref[:, half:] = below[:, :half]
    dn2_ref[...] = below[:, half:]
    mine_ref[...] = term(0)


def expert_backward(rank, gots, slope, weights, n_tp):
    rows = gots[0].shape[0]
    hidden, width = weights[0].shape
    part = width // n_tp
    fetched = len(weights) == 3
    block = 384 if rows % 384 == 0 and not fetched else 256
    by_rows = lambda cols: pl.BlockSpec((block, cols), lambda i: (i, 0))
    whole = pl.BlockSpec(memory_space=pl.ANY if fetched else pltpu.VMEM)
    scratch = [
        pltpu.VMEM((hidden, width), BF),
        pltpu.VMEM((width, 2 * hidden), BF),
        pltpu.SemaphoreType.DMA((n_tp + 2,)),
    ]
    if fetched:
        slope, *weights = in_hbm(slope, *weights)
    outs = (2 * hidden, part, part, part // 2, part // 2, part)
    return pl.pallas_call(
        functools.partial(backward_kernel, count=len(gots), fetched=fetched, n_tp=n_tp),
        grid=(rows // block,),
        in_specs=[pl.BlockSpec(memory_space=pltpu.SMEM)]
        + [by_rows(g.shape[1]) for g in gots]
        + [by_rows(2 * hidden)]
        + [whole] * len(weights),
        out_specs=tuple(by_rows(c) for c in outs),
        out_shape=tuple(hbm((rows, c)) for c in outs),
        scratch_shapes=scratch if fetched else [],
        compiler_params=params(24),
        name="expert_backward",
    )(rank, *gots, slope, *weights)


def summed_products(lefts, rights):
    total = None
    for left, right in zip(lefts, rights):
        term = lax.dot_general(left[...], right[...], COLS_COLS, preferred_element_type=F32)
        total = term if total is None else total + term
    return total


def gate_up_kernel(*refs, groups):
    gate_ref, up_ref = refs[2 * groups :]
    total = summed_products(refs[:groups], refs[groups : 2 * groups])
    hidden = gate_ref.shape[1]
    gate_ref[...] = total[:, :hidden].astype(BF)
    up_ref[...] = total[:, hidden:].astype(BF)


def gate_up_grads(saved, both):
    width, hidden = saved[0].shape[1], both[0].shape[1] // 2
    block = 512
    out = pl.BlockSpec((block, hidden), lambda i: (i, 0))
    return pl.pallas_call(
        functools.partial(gate_up_kernel, groups=len(saved)),
        grid=(width // block,),
        in_specs=[pl.BlockSpec((x.shape[0], block), lambda i: (0, i)) for x in saved]
        + [pl.BlockSpec(g.shape, lambda i: (0, 0)) for g in both],
        out_specs=(out, out),
        out_shape=(jax.ShapeDtypeStruct((width, hidden), BF),) * 2,
        compiler_params=params(32),
        name="gate_up_grads",
    )(*in_hbm(*saved, *both))


def down_kernel(rank_ref, first_act, second_act, second, *refs, count, n_tp):
    pieces, refs = refs[:count], refs[count:]
    out_ref, act0, act1, rows0, rows1, turned0, turned1, sems = refs
    part = second.shape[1] // n_tp
    half = part // 2
    pairs = [(first_act, act0), (second_act, act1), (second, rows1)]
    for i, piece in enumerate(pieces):
        ahead, side = (0, 0) if i == 0 else ((i + 1) // 2, (i + 1) % 2)
        at = lax.rem(rank_ref[0] + ahead, n_tp) * part + side * half
        columns = pl.ds(pl.multiple_of(at, half), piece.shape[1])
        pairs.append((piece, rows0.at[:, columns]))
    copies = [pltpu.make_async_copy(a, b, sems.at[i]) for i, (a, b) in enumerate(pairs)]
    for copy in copies:
        copy.start()
    for copy in copies[:2]:
        copy.wait()
    turned0[...] = act0[...].T
    turned1[...] = act1[...].T
    for copy in copies[2:]:
        copy.wait()
    for m in range(n_tp):
        columns = slice(m * part, (m + 1) * part)
        total = jnp.dot(turned0[...], rows0[:, columns], preferred_element_type=F32)
        total = total + jnp.dot(turned1[...], rows1[:, columns], preferred_element_type=F32)
        out_ref[:, columns] = total.astype(BF)


def down_grads(rank, acts, received, n_tp):
    pieces, (second,) = received
    arrays = (*acts, second, *pieces)
    hidden, width = acts[0].shape[1], second.shape[1]
    counts = [a.shape[0] for a in acts]
    return pl.pallas_call(
        functools.partial(down_kernel, count=len(pieces), n_tp=n_tp),
        grid=(1,),
        in_specs=[pl.BlockSpec(memory_space=pltpu.SMEM)]
        + [pl.BlockSpec(memory_space=pl.ANY)] * len(arrays),
        out_specs=pl.BlockSpec((hidden, width), lambda i: (0, 0)),
        out_shape=hbm((hidden, width)),
        scratch_shapes=[pltpu.VMEM((n, hidden), BF) for n in counts]
        + [pltpu.VMEM((n, width), BF) for n in counts]
        + [pltpu.VMEM((hidden, n), BF) for n in counts]
        + [pltpu.SemaphoreType.DMA((len(arrays),))],
        compiler_params=params(32),
        name="down_grads",
    )(rank, *in_hbm(*arrays))


def ring(n, step):
    return [(i, (i + step) % n) for i in range(n)]


def gathered_over_tp(x, n_tp):
    half = x.shape[1] // 2
    below = lax.ppermute(x, "tp", ring(n_tp, 1))
    above = lax.ppermute(x, "tp", ring(n_tp, -1))
    left, right = below[:, :half], above[:, half:]
    left = lax.ppermute(left, "tp", ring(n_tp, 1))
    right = lax.ppermute(right, "tp", ring(n_tp, -1))
    return below, above, left, right


def gathered_early(x, n_tp):
    half = x.shape[1] // 2
    left, right = x[:, :half], x[:, half:]
    up, down = ring(n_tp, 1), ring(n_tp, -1)
    below_left = lax.ppermute(left, "tp", up)
    above_right = lax.ppermute(right, "tp", down)
    below_right = lax.ppermute(right, "tp", up)
    above_left = lax.ppermute(left, "tp", down)
    away_left = lax.ppermute(below_left, "tp", up)
    away_right = lax.ppermute(above_right, "tp", down)
    return (x, above_left, above_right, away_left, away_right, below_left, below_right)


def summed_over_tp(up1, dn1, up2, dn2, mine, n_tp):
    half = up2.shape[1]
    from_below = lax.ppermute(up1, "tp", ring(n_tp, 1))
    from_above = lax.ppermute(dn1, "tp", ring(n_tp, -1))
    add = lambda a, b: (a.astype(F32) + b.astype(F32)).astype(BF)
    up2 = add(up2, from_below[:, :half])
    dn2 = add(dn2, from_above[:, :half])
    left = lax.ppermute(up2, "tp", ring(n_tp, 1))
    right = lax.ppermute(dn2, "tp", ring(n_tp, -1))
    far = jnp.concatenate([left, right], axis=1).astype(F32)
    near = jnp.concatenate([from_above[:, half:], from_below[:, half:]], axis=1).astype(F32)
    return (mine.astype(F32) + far + near).astype(BF)


def combine_kernel(col_ref, cot_ref, back_ref, out_ref):
    tokens, top = col_ref.shape
    at = iota((tokens, back_ref.shape[0]), 1)
    hit = col_ref[:, 0:1] == at
    for k in range(1, top):
        hit = hit | (col_ref[:, k : k + 1] == at)
    total = jnp.dot(hit.astype(F32).astype(BF), back_ref[...], preferred_element_type=F32)
    out_ref[...] = (cot_ref[...].astype(F32) + total).astype(BF)


def combine(col, cot_part, back):
    return pl.pallas_call(
        combine_kernel,
        out_shape=jax.ShapeDtypeStruct(cot_part.shape, BF),
        compiler_params=params(16),
        name="combine",
    )(col, cot_part, back)


def pieces_of(rank_ref, z_refs, n_tp):
    z0, z_below, z_above, z_top, z_bottom = z_refs
    me = rank_ref[0]
    away = jnp.concatenate([z_top[...], z_bottom[...]], axis=1)
    order = ((0, z0[...]), (n_tp - 1, z_below[...]), (1, z_above[...]), (2, away))
    width = z0.shape[1]
    return [(pl.multiple_of(lax.rem(me + a, n_tp) * width, width), z) for a, z in order]


def state_kernel(
    rank_ref,
    z0,
    z1,
    z2,
    z3,
    z4,
    w_hbm,
    mixed_ref,
    branch_ref,
    decay_ref,
    later_ref,
    earlier_ref,
    branch_grad_ref,
    state_ref,
    carry_ref,
    w_ref,
    sem,
    *,
    n_tp,
):
    copy = pltpu.make_async_copy(w_hbm, w_ref, sem)
    copy.start()
    copy.wait()
    total = None
    for at, z in pieces_of(rank_ref, (z0, z1, z2, z3, z4), n_tp):
        term = jnp.dot(z, w_ref[pl.ds(at, z.shape[1]), :], preferred_element_type=F32)
        total = term if total is None else total + term
    branch_grad_ref[...] = (total * mixed_ref[...].astype(F32)).astype(BF)
    state = total * branch_ref[...].astype(F32)
    state_ref[...] = state
    scaled = state * decay_ref[...]
    ahead = jnp.sum(scaled * earlier_ref[...], axis=0, keepdims=True)
    behind = jnp.sum(scaled * later_ref[...], axis=0, keepdims=True)
    last = slice(state.shape[0] - 1, state.shape[0])
    through = decay_ref[last, :] * earlier_ref[last, :]
    lanes = carry_ref.shape[2]
    count = ahead.shape[1] // lanes
    tile = jnp.concatenate(
        [
            v[:, b * lanes : (b + 1) * lanes]
            for v in (ahead, behind, through, through)
            for b in range(count)
        ],
        axis=0,
    )
    carry_ref[...] = jnp.broadcast_to(tile[None], carry_ref.shape)


def state_grads(rank, zs, w_out, mixed, branch, decay, later_prod, earlier_prod, n_sp, n_tp):
    tokens, channels = mixed.shape
    full = lambda *shape: pl.BlockSpec(shape, lambda i: (0,) * len(shape))
    held = full(tokens, channels)
    carry = (n_sp, 16, channels // 4)
    return pl.pallas_call(
        functools.partial(state_kernel, n_tp=n_tp),
        grid=(1,),
        in_specs=[pl.BlockSpec(memory_space=pltpu.SMEM)]
        + [full(*z.shape) for z in zs]
        + [pl.BlockSpec(memory_space=pl.ANY)]
        + [held] * 5,
        out_specs=(held, held, full(*carry)),
        out_shape=(hbm((tokens, channels)), hbm((tokens, channels), F32), hbm(carry, F32)),
        scratch_shapes=[pltpu.VMEM(w_out.shape, BF), pltpu.SemaphoreType.DMA(())],
        compiler_params=params(32),
        name="state_grads",
    )(rank, *zs, *in_hbm(w_out, mixed, branch, decay, later_prod, earlier_prod))


def proj_kernel(rank_ref, core_ref, z_ref, own, above, left, right, below, keep_ref, send_ref, *, n_tp, size):
    z = z_ref[...]
    me = rank_ref[0]
    same = lax.rem(me + core_ref[0], 2) == 0

    def term(ahead):
        if ahead == 2:
            channels = jnp.concatenate([left[...], right[...]], axis=1)
        else:
            channels = {0: own, 1: above, 3: below}[ahead][...]
        return lax.dot_general(z, channels, COLS_COLS, preferred_element_type=F32).astype(BF)

    for a, b in ((0, 1), (2, 3)):
        first, second = term(a), term(b)
        at = [lax.rem(me + ahead, n_tp) // 2 for ahead in (a, b)]
        kept = jnp.where(same, at[0], at[1]) * size
        sent = jnp.where(same, at[1], at[0]) * size
        for i in range(first.shape[0] // size):
            rows = slice(i * size, (i + 1) * size)
            base = i * (n_tp // 2) * size
            keep_ref[pl.ds(pl.multiple_of(base + kept, size), size), :] = jnp.where(
                same, first[rows], second[rows]
            )
            send_ref[pl.ds(pl.multiple_of(base + sent, size), size), :] = jnp.where(
                same, second[rows], first[rows]
            )


def proj_terms(rank, core, z, gateds, n_tp, n_sp):
    features, channels = z.shape[1], gateds[0].shape[1]
    size = features * n_tp // n_sp
    half = jax.ShapeDtypeStruct((features * n_tp // 2, channels), BF)
    return pl.pallas_call(
        functools.partial(proj_kernel, n_tp=n_tp, size=size),
        in_specs=[pl.BlockSpec(memory_space=pltpu.SMEM)] * 2
        + [pl.BlockSpec(memory_space=pltpu.VMEM)] * 6,
        out_shape=(half, half),
        compiler_params=params(20),
        name="proj_terms",
    )(rank, core, z, *gateds)


def carried_in(me, got_ref):
    count, half = got_ref.shape[0], got_ref.shape[1] // 2
    carry = lambda q: got_ref[q, :half, :]
    through = lambda q: got_ref[q, half:, :]
    zero = jnp.zeros((half, got_ref.shape[2]), F32)
    ahead, behind = zero, zero
    for q in range(count):
        p = count - 1 - q
        ahead = jnp.where(p > me, carry(p) + through(p) * ahead, ahead)
        behind = jnp.where(q < me, carry(q) + through(q) * behind, behind)
    return ahead[: half // 2], behind[half // 2 :]


def final_kernel(me_ref, got_ref, *refs):
    sources, out_ref = refs[:8], refs[8]
    later_ref, earlier_ref = refs[9:11]
    holds, sems = refs[11:19], refs[19]
    copies = [pltpu.make_async_copy(a, b, sems.at[i]) for i, (a, b) in enumerate(zip(sources, holds))]
    for copy in copies:
        copy.start()
    for copy in copies[:2]:
        copy.wait()
    state_ref, decay_ref, h_later, h_earlier, q_ref, r_ref, rec_w, inp_w = holds
    rows = state_ref.shape[0]
    ahead, behind = carried_in(me_ref[0], got_ref)
    spread = lambda v: jnp.concatenate([v[b : b + 1] for b in range(v.shape[0])], axis=1)

    def step(i, carry):
        ahead, behind = carry
        t = rows - 1 - i
        later = state_ref[pl.ds(t, 1), :] + ahead
        later_ref[pl.ds(t, 1), :] = later
        earlier = state_ref[pl.ds(i, 1), :] + behind
        earlier_ref[pl.ds(i, 1), :] = earlier
        return (later * decay_ref[pl.ds(t, 1), :], earlier * decay_ref[pl.ds(i, 1), :])

    lax.fori_loop(0, rows, step, (spread(ahead), spread(behind)), unroll=8)
    for copy in copies[2:]:
        copy.wait()
    later, earlier = later_ref[...], earlier_ref[...]
    total = later + earlier
    h_later, h_earlier = h_later[...].astype(F32), h_earlier[...].astype(F32)
    rec_pre = (later * h_later + earlier * h_earlier).astype(BF)
    inp_pre = (total * q_ref[...].astype(F32)).astype(BF)
    direct = total * r_ref[...].astype(F32)
    size = rec_w.shape[1]
    for b in range(rec_w.shape[0]):
        cols = slice(b * size, (b + 1) * size)
        term = lax.dot_general(rec_pre[:, cols], rec_w[b], ROWS_ROWS, preferred_element_type=F32)
        term = term + lax.dot_general(
            inp_pre[:, cols], inp_w[b], ROWS_ROWS, preferred_element_type=F32
        )
        out_ref[:, cols] = (direct[:, cols] + term).astype(BF)


def final_grads(me, got, arrays, rec_w, inp_w):
    tokens, channels = arrays[0].shape
    sources = (*arrays, rec_w, inp_w)
    return pl.pallas_call(
        final_kernel,
        grid=(1,),
        in_specs=[
            pl.BlockSpec(memory_space=pltpu.SMEM),
            pl.BlockSpec(got.shape, lambda i: (0, 0, 0)),
        ]
        + [pl.BlockSpec(memory_space=pl.ANY)] * len(sources),
        out_specs=pl.BlockSpec((tokens, channels), lambda i: (0, 0)),
        out_shape=hbm((tokens, channels)),
        scratch_shapes=[pltpu.VMEM((tokens, channels), F32)] * 2
        + [pltpu.VMEM(a.shape, a.dtype) for a in sources]
        + [pltpu.SemaphoreType.DMA((len(sources),))],
        compiler_params=params(24),
        name="final_grads",
    )(me, got, *in_hbm(*sources))


def blockwise(rows, weights):
    size = weights.shape[1]
    return jnp.concatenate(
        [
            jnp.dot(rows[:, b * size : (b + 1) * size], weights[b], preferred_element_type=F32)
            for b in range(weights.shape[0])
        ],
        axis=1,
    )


def shards(
    output_cotangent,
    chosen_expert_index,
    chosen_expert_weight,
    expert_slot_tokens,
    expert_gate_matrix,
    expert_up_matrix,
    expert_down_matrix,
    output_projection_matrix,
    recurrence_input,
    branch_activation_values,
    forward_scan_state,
    reverse_scan_state,
    channel_decay_rate,
    position_extra_log_decay,
    recurrence_gate_weights,
    input_gate_weights,
):
    n_sp = lax.axis_size("sp")
    n_tp = lax.axis_size("tp")
    tokens, model_width = output_cotangent.shape
    experts = n_sp * expert_gate_matrix.shape[0]
    capacity = expert_slot_tokens.shape[1] // n_sp
    slots = expert_slot_tokens.shape[1]
    hidden = expert_gate_matrix.shape[2]
    part = model_width // n_tp
    rank = lax.axis_index("tp").astype(jnp.int32).reshape(1)
    place = lax.axis_index("sp").astype(jnp.int32).reshape(1)
    bounds, at = [], 0
    for size in SLOT_GROUPS:
        bounds.append((at, size))
        at += size

    chosen_t, weight_t = chosen_expert_index.T, chosen_expert_weight.T
    w_gate, w_up, w_down = expert_gate_matrix[0], expert_up_matrix[0], expert_down_matrix[0]
    received = []
    for g, (base, size) in enumerate(bounds):
        width = model_width if g else part
        column = jnp.zeros_like(rank) if g else rank
        out = dispatch(
            column,
            chosen_t,
            weight_t,
            output_cotangent if g else in_hbm(output_cotangent)[0],
            width,
            base * experts,
            size * experts,
            experts,
        )
        got = lax.all_to_all(out.reshape(experts, size, -1), "sp", 0, 0, tiled=True)
        got = got.reshape(n_sp * size, -1)
        if g:
            received.append((got,))
        else:
            received.append(gathered_early(got, n_tp))
    down_turned, w_cat = fetched_weights(rank, w_down, w_gate, w_up, n_tp)

    by_source = expert_slot_tokens.reshape(n_sp, capacity, model_width)
    saved, acts, slopes = [], [], []
    for g, (base, size) in enumerate(bounds):
        x = by_source[:, base : base + size].reshape(n_sp * size, model_width)
        act, slope = expert_forward(x, (w_cat,) if g else (w_gate, w_up), hidden)
        saved.append(x)
        acts.append(act)
        slopes.append(slope)

    rec = jax.nn.sigmoid(blockwise(recurrence_input, recurrence_gate_weights))
    inp = jax.nn.sigmoid(blockwise(recurrence_input, input_gate_weights))
    rate = -gate_scale_factor * channel_decay_rate[None, :]
    log_decay = rec * rate + position_extra_log_decay[:, None]
    decay = jnp.exp(log_decay)
    scale_in = jnp.sqrt(-jnp.expm1(2.0 * log_decay))
    inputs = recurrence_input.astype(F32)
    xin = scale_in * inp * inputs
    mixed = (
        (decay * forward_scan_state + xin) + (decay * reverse_scan_state + xin)
    ).astype(BF)
    gated = (mixed.astype(F32) * branch_activation_values.astype(F32)).astype(BF)
    lower = (iota((tokens, tokens), 1) <= iota((tokens, tokens), 0)).astype(F32)
    running = jnp.dot(lower, log_decay, precision=lax.Precision.HIGHEST)
    later_prod = jnp.exp(running[-1:] - running)
    earlier_prod = jnp.exp(running - log_decay)
    rec_slope = rate * rec * (1.0 - rec)
    shared = inp * inputs * decay * decay / scale_in
    h_later = ((forward_scan_state * decay - shared) * rec_slope).astype(BF)
    h_earlier = ((reverse_scan_state * decay - shared) * rec_slope).astype(BF)
    q = (scale_in * inputs * inp * (1.0 - inp)).astype(BF)
    r = (scale_in * inp).astype(BF)

    boths, sums = [], []
    for g, (base, size) in enumerate(bounds):
        weights = (w_down, w_gate, w_up) if g else (down_turned, w_cat)
        both, *terms = expert_backward(rank, received[g], slopes[g], weights, n_tp)
        sums.append(summed_over_tp(*terms, n_tp).reshape(n_sp, size, part))
        boths.append(both)
    back = lax.all_to_all(jnp.concatenate(sums, axis=1), "sp", 0, 0, tiled=True)
    gate_grad, up_grad = gate_up_grads(saved, boths)
    down_grad = down_grads(rank, acts, received, n_tp)

    below, above, left, right = gathered_over_tp(gated, n_tp)
    gateds = (gated, above, left, right, below)

    cot_part = lax.dynamic_slice_in_dim(output_cotangent, rank[0] * part, part, 1)
    col = slot_columns(chosen_expert_index, experts)
    z0 = combine(col, cot_part, back.reshape(slots, part))
    zs = (z0, *gathered_over_tp(z0, n_tp))

    keep, send = proj_terms(rank, place % 2, z0, gateds, n_tp, n_sp)
    other = lax.ppermute(send, "sp", [(i, i ^ 1) for i in range(n_sp)])
    terms = (keep.astype(F32) + other.astype(F32)).astype(BF)
    terms = terms.reshape(n_sp // 2, model_width // n_sp, -1)
    groups = [list(range(c, n_sp, 2)) for c in range(2)]
    terms = lax.all_to_all(terms, "sp", 0, 0, axis_index_groups=groups, tiled=True)
    proj_grad = jnp.sum(terms.astype(F32), axis=0)
    spread = n_sp // n_tp
    moves = [
        (s * n_tp + x, (x * spread + s // n_tp) * n_tp + s % n_tp)
        for s in range(n_sp)
        for x in range(n_tp)
    ]
    proj_grad = lax.ppermute(proj_grad, ("sp", "tp"), moves)

    branch_grad, state, carry = state_grads(
        rank,
        zs,
        output_projection_matrix,
        mixed,
        branch_activation_values,
        decay,
        later_prod,
        earlier_prod,
        n_sp,
        n_tp,
    )
    carried = lax.all_to_all(carry, "sp", 0, 0, tiled=True)
    input_grad = final_grads(
        place,
        carried,
        (state, decay, h_later, h_earlier, q, r),
        recurrence_gate_weights,
        input_gate_weights,
    )
    return (gate_grad[None], up_grad[None], down_grad[None], proj_grad, branch_grad, input_grad)


def solution(mesh):
    in_specs = (
        P("sp", None),
        P("sp", None),
        P("sp", None),
        P("sp", None, None),
        P("sp", None, "tp"),
        P("sp", None, "tp"),
        P("sp", "tp", None),
        P(None, "tp"),
        P("sp", "tp"),
        P("sp", "tp"),
        P("sp", "tp"),
        P("sp", "tp"),
        P("tp"),
        P("sp"),
        P("tp", None, None),
        P("tp", None, None),
    )
    out_specs = (
        P("sp", None, "tp"),
        P("sp", None, "tp"),
        P("sp", "tp", None),
        P("sp", "tp"),
        P("sp", "tp"),
        P("sp", "tp"),
    )
    return jax.shard_map(shards, mesh=mesh, in_specs=in_specs, out_specs=out_specs, check_vma=False)
```

```python
import functools

import jax
import jax.numpy as jnp
from jax import lax
from jax.experimental import pallas as pl
from jax.experimental.pallas import tpu as pltpu
from jax.sharding import PartitionSpec as P


gate_scale_factor = 8.0
clamp_limit = 7.0
glu_alpha = 1.702

BF = jnp.bfloat16
F32 = jnp.float32

SLOT_GROUPS = (24, 16)

ROWS_ROWS = (((1,), (1,)), ((), ()))
COLS_COLS = (((0,), (0,)), ((), ()))


def params(limit_mib):
    return pltpu.CompilerParams(vmem_limit_bytes=limit_mib * 1024 * 1024)


def hbm(shape, dtype=BF):
    return pltpu.HBM(shape, dtype)


def in_hbm(*arrays):
    return tuple(pltpu.with_memory_space_constraint(a, pltpu.HBM) for a in arrays)


def iota(shape, dim):
    return lax.broadcasted_iota(jnp.int32, shape, dim)


def placed_row(expert, slot, experts):
    base, row = 0, None
    for size in SLOT_GROUPS:
        here = base * experts + expert * size + (slot - base)
        row = here if row is None else jnp.where(slot >= base, here, row)
        base += size
    return row


def slots_kernel(idx_ref, col_ref, *, experts):
    tokens, top = idx_ref.shape
    a, b = iota((tokens, tokens), 0), iota((tokens, tokens), 1)
    hot = [idx_ref[:, k : k + 1] == iota((tokens, experts), 1) for k in range(top)]
    both = sum(h.astype(F32) for h in hot).astype(BF)
    before = jnp.dot((b < a).astype(F32).astype(BF), both, preferred_element_type=F32)
    for k in range(top):
        rank = jnp.sum(jnp.where(hot[k], before, 0.0), axis=1, keepdims=True).astype(jnp.int32)
        col_ref[:, k : k + 1] = idx_ref[:, k : k + 1] * sum(SLOT_GROUPS) + rank


def slot_columns(chosen, experts):
    return pl.pallas_call(
        functools.partial(slots_kernel, experts=experts),
        out_shape=jax.ShapeDtypeStruct(chosen.shape, jnp.int32),
        compiler_params=params(8),
        name="slots",
    )(chosen)


def dispatch_kernel(_, idx_ref, weight_ref, cot_ref, out_ref, row_ref, *, first, experts):
    rows, tokens = out_ref.shape[0], cot_ref.shape[0]
    top = idx_ref.shape[0]

    @pl.when(pl.program_id(0) == 0)
    def _():
        a, b = iota((tokens, tokens), 0), iota((tokens, tokens), 1)
        hot = [idx_ref[k : k + 1, :] == iota((experts, tokens), 0) for k in range(top)]
        both = sum(h.astype(F32) for h in hot).astype(BF)
        before = jnp.dot(both, (a < b).astype(F32).astype(BF), preferred_element_type=F32)
        for k in range(top):
            rank = jnp.sum(jnp.where(hot[k], before, 0.0), axis=0, keepdims=True)
            row_ref[k : k + 1, :] = placed_row(
                idx_ref[k : k + 1, :], rank.astype(jnp.int32), experts
            )

    at = first + pl.program_id(0) * rows + iota((rows, tokens), 0)
    weight = jnp.zeros((rows, tokens), F32)
    for k in range(top):
        weight = jnp.where(row_ref[k : k + 1, :] == at, weight_ref[k : k + 1, :], weight)
    picked = jnp.dot((weight > 0.0).astype(F32).astype(BF), cot_ref[...], preferred_element_type=F32)
    out_ref[...] = (picked * jnp.sum(weight, axis=1, keepdims=True)).astype(BF)


def dispatch(column, chosen_t, weight_t, cot, width, first, count, experts):
    block = 256
    return pl.pallas_call(
        functools.partial(dispatch_kernel, first=first, experts=experts),
        grid_spec=pltpu.PrefetchScalarGridSpec(
            num_scalar_prefetch=1,
            grid=(count // block,),
            in_specs=[
                pl.BlockSpec(chosen_t.shape, lambda i, c: (0, 0)),
                pl.BlockSpec(weight_t.shape, lambda i, c: (0, 0)),
                pl.BlockSpec((cot.shape[0], width), lambda i, c: (0, c[0])),
            ],
            out_specs=pl.BlockSpec((block, width), lambda i, c: (i, 0)),
            scratch_shapes=[pltpu.VMEM(chosen_t.shape, jnp.int32)],
        ),
        out_shape=hbm((count, width)),
        compiler_params=params(12),
        name="dispatch",
    )(column, chosen_t, weight_t, cot)


def weight_copies(rank, down, gate, up, down_to, cat_to, sems, n_tp, cat_only=False):
    hidden, part = gate.shape[1], down.shape[1] // n_tp
    copies = []
    for m in range(n_tp):
        at = pl.multiple_of(lax.rem(rank + m, n_tp) * part, part)
        copies.append((down.at[:, pl.ds(at, part)], down_to.at[:, m * part : (m + 1) * part]))
    copies.append((gate, cat_to.at[:, :hidden]))
    copies.append((up, cat_to.at[:, hidden:]))
    first = n_tp if cat_only else 0
    return [
        pltpu.make_async_copy(a, b, sems.at[first + i])
        for i, (a, b) in enumerate(copies[first:])
    ]


def fetch_kernel(rank_ref, down, gate, up, down_to, cat_to, sems, *, n_tp):
    copies = weight_copies(rank_ref[0], down, gate, up, down_to, cat_to, sems, n_tp)
    for copy in copies:
        copy.start()
    for copy in copies:
        copy.wait()


def fetched_weights(rank, w_down, w_gate, w_up, n_tp):
    width, hidden = w_gate.shape
    return pl.pallas_call(
        functools.partial(fetch_kernel, n_tp=n_tp),
        in_specs=[pl.BlockSpec(memory_space=pltpu.SMEM)]
        + [pl.BlockSpec(memory_space=pl.ANY)] * 3,
        out_specs=(pl.BlockSpec(memory_space=pltpu.VMEM),) * 2,
        out_shape=(pltpu.VMEM(w_down.shape, BF), pltpu.VMEM((width, 2 * hidden), BF)),
        scratch_shapes=[pltpu.SemaphoreType.DMA((n_tp + 2,))],
        compiler_params=params(4),
        name="fetch",
    )(rank, *in_hbm(w_down, w_gate, w_up))


def forward_kernel(x_ref, *refs):
    weights, (act_ref, slope_ref) = refs[:-2], refs[-2:]
    x = x_ref[...]
    hidden = act_ref.shape[1]
    pre = [jnp.dot(x, w[...], preferred_element_type=F32) for w in weights]
    gate_pre, up_pre = pre if len(pre) == 2 else (pre[0][:, :hidden], pre[0][:, hidden:])
    glu = jnp.minimum(gate_pre, clamp_limit)
    lin = jnp.clip(up_pre, -clamp_limit, clamp_limit) + 1.0
    sig = 1.0 / (1.0 + jnp.exp(-glu_alpha * glu))
    silu = glu * sig
    act_ref[...] = (silu * lin).astype(BF)
    slope = lin * (sig + glu_alpha * silu * (1.0 - sig))
    slope_ref[:, :hidden] = jnp.where(gate_pre < clamp_limit, slope, 0.0)
    slope_ref[:, hidden:] = jnp.where(jnp.abs(up_pre) < clamp_limit, silu, 0.0)


def expert_forward(x, weights, hidden):
    rows, width = x.shape
    block = 384 if rows % 384 == 0 else 256
    whole = pl.BlockSpec(memory_space=pltpu.VMEM)
    return pl.pallas_call(
        forward_kernel,
        grid=(rows // block,),
        in_specs=[pl.BlockSpec((block, width), lambda i: (i, 0))] + [whole] * len(weights),
        out_specs=(
            pl.BlockSpec((block, hidden), lambda i: (i, 0)),
            pl.BlockSpec((block, 2 * hidden), lambda i: (i, 0)),
        ),
        out_shape=(hbm((rows, hidden)), hbm((rows, 2 * hidden), F32)),
        compiler_params=params(24),
        name="expert_forward",
    )(x, *weights)


def backward_kernel(rank_ref, *refs, count, fetched, n_tp):
    got_refs, refs = refs[:count], refs[count:]
    slope_ref, refs = refs[0], refs[1:]
    sources, refs = (refs[:3], refs[3:]) if fetched else ((), refs)
    weights, refs = ((), refs) if fetched else (refs[:2], refs[2:])
    both_ref, up1_ref, dn1_ref, up2_ref, dn2_ref, mine_ref = refs[:6]
    first = pl.program_id(0) == 0
    if fetched:
        weights, sems = refs[6:8], refs[8]

        @pl.when(first)
        def _():
            copies = weight_copies(0, *sources, *weights, sems, n_tp)
            for copy in copies:
                copy.start()
            for copy in copies[:n_tp]:
                copy.wait()

    down_ref, cat_ref = weights
    width = mine_ref.shape[1]
    half = width // 2
    hidden = down_ref.shape[0]
    got = [ref[...] for ref in got_refs]
    got = got[0] if len(got) == 1 else jnp.concatenate(got, axis=1)
    d_act = lax.dot_general(got, down_ref[...], ROWS_ROWS, preferred_element_type=F32)
    both_ref[:, :hidden] = (d_act * slope_ref[:, :hidden]).astype(BF)
    both_ref[:, hidden:] = (d_act * slope_ref[:, hidden:]).astype(BF)
    if fetched:

        @pl.when(first)
        def _():
            for copy in weight_copies(0, *sources, *weights, sems, n_tp, True):
                copy.wait()

    both = both_ref[...]

    def term(ahead):
        at = pl.multiple_of(lax.rem(rank_ref[0] + ahead, n_tp) * width, width)
        return lax.dot_general(
            both, cat_ref[pl.ds(at, width), :], ROWS_ROWS, preferred_element_type=F32
        ).astype(BF)

    away = term(2)
    up1_ref[:, :half] = away[:, :half]
    dn1_ref[:, :half] = away[:, half:]
    above = term(1)
    up1_ref[:, half:] = above[:, half:]
    up2_ref[...] = above[:, :half]
    below = term(3)
    dn1_ref[:, half:] = below[:, :half]
    dn2_ref[...] = below[:, half:]
    mine_ref[...] = term(0)


def expert_backward(rank, gots, slope, weights, n_tp):
    rows = gots[0].shape[0]
    hidden, width = weights[0].shape
    part = width // n_tp
    fetched = len(weights) == 3
    block = 384 if rows % 384 == 0 and not fetched else 256
    by_rows = lambda cols: pl.BlockSpec((block, cols), lambda i: (i, 0))
    whole = pl.BlockSpec(memory_space=pl.ANY if fetched else pltpu.VMEM)
    scratch = [
        pltpu.VMEM((hidden, width), BF),
        pltpu.VMEM((width, 2 * hidden), BF),
        pltpu.SemaphoreType.DMA((n_tp + 2,)),
    ]
    if fetched:
        slope, *weights = in_hbm(slope, *weights)
    outs = (2 * hidden, part, part, part // 2, part // 2, part)
    return pl.pallas_call(
        functools.partial(backward_kernel, count=len(gots), fetched=fetched, n_tp=n_tp),
        grid=(rows // block,),
        in_specs=[pl.BlockSpec(memory_space=pltpu.SMEM)]
        + [by_rows(g.shape[1]) for g in gots]
        + [by_rows(2 * hidden)]
        + [whole] * len(weights),
        out_specs=tuple(by_rows(c) for c in outs),
        out_shape=tuple(hbm((rows, c)) for c in outs),
        scratch_shapes=scratch if fetched else [],
        compiler_params=params(24),
        name="expert_backward",
    )(rank, *gots, slope, *weights)


def summed_products(lefts, rights):
    total = None
    for left, right in zip(lefts, rights):
        term = lax.dot_general(left[...], right[...], COLS_COLS, preferred_element_type=F32)
        total = term if total is None else total + term
    return total


def gate_up_kernel(*refs, groups):
    gate_ref, up_ref = refs[2 * groups :]
    total = summed_products(refs[:groups], refs[groups : 2 * groups])
    hidden = gate_ref.shape[1]
    gate_ref[...] = total[:, :hidden].astype(BF)
    up_ref[...] = total[:, hidden:].astype(BF)


def gate_up_grads(saved, both):
    width, hidden = saved[0].shape[1], both[0].shape[1] // 2
    block = 512
    out = pl.BlockSpec((block, hidden), lambda i: (i, 0))
    return pl.pallas_call(
        functools.partial(gate_up_kernel, groups=len(saved)),
        grid=(width // block,),
        in_specs=[pl.BlockSpec((x.shape[0], block), lambda i: (0, i)) for x in saved]
        + [pl.BlockSpec(g.shape, lambda i: (0, 0)) for g in both],
        out_specs=(out, out),
        out_shape=(jax.ShapeDtypeStruct((width, hidden), BF),) * 2,
        compiler_params=params(32),
        name="gate_up_grads",
    )(*in_hbm(*saved, *both))


def down_kernel(rank_ref, first_act, second_act, second, *refs, count, n_tp):
    pieces, refs = refs[:count], refs[count:]
    out_ref, act0, act1, rows0, rows1, turned0, turned1, sems = refs
    part = second.shape[1] // n_tp
    half = part // 2
    pairs = [(first_act, act0), (second_act, act1), (second, rows1)]
    for i, piece in enumerate(pieces):
        ahead, side = (0, 0) if i == 0 else ((i + 1) // 2, (i + 1) % 2)
        at = lax.rem(rank_ref[0] + ahead, n_tp) * part + side * half
        columns = pl.ds(pl.multiple_of(at, half), piece.shape[1])
        pairs.append((piece, rows0.at[:, columns]))
    copies = [pltpu.make_async_copy(a, b, sems.at[i]) for i, (a, b) in enumerate(pairs)]
    for copy in copies:
        copy.start()
    for copy in copies[:2]:
        copy.wait()
    turned0[...] = act0[...].T
    turned1[...] = act1[...].T
    for copy in copies[2:]:
        copy.wait()
    for m in range(n_tp):
        columns = slice(m * part, (m + 1) * part)
        total = jnp.dot(turned0[...], rows0[:, columns], preferred_element_type=F32)
        total = total + jnp.dot(turned1[...], rows1[:, columns], preferred_element_type=F32)
        out_ref[:, columns] = total.astype(BF)


def down_grads(rank, acts, received, n_tp):
    pieces, (second,) = received
    arrays = (*acts, second, *pieces)
    hidden, width = acts[0].shape[1], second.shape[1]
    counts = [a.shape[0] for a in acts]
    return pl.pallas_call(
        functools.partial(down_kernel, count=len(pieces), n_tp=n_tp),
        grid=(1,),
        in_specs=[pl.BlockSpec(memory_space=pltpu.SMEM)]
        + [pl.BlockSpec(memory_space=pl.ANY)] * len(arrays),
        out_specs=pl.BlockSpec((hidden, width), lambda i: (0, 0)),
        out_shape=hbm((hidden, width)),
        scratch_shapes=[pltpu.VMEM((n, hidden), BF) for n in counts]
        + [pltpu.VMEM((n, width), BF) for n in counts]
        + [pltpu.VMEM((hidden, n), BF) for n in counts]
        + [pltpu.SemaphoreType.DMA((len(arrays),))],
        compiler_params=params(32),
        name="down_grads",
    )(rank, *in_hbm(*arrays))


def ring(n, step):
    return [(i, (i + step) % n) for i in range(n)]


def gathered_over_tp(x, n_tp):
    half = x.shape[1] // 2
    below = lax.ppermute(x, "tp", ring(n_tp, 1))
    above = lax.ppermute(x, "tp", ring(n_tp, -1))
    left, right = below[:, :half], above[:, half:]
    left = lax.ppermute(left, "tp", ring(n_tp, 1))
    right = lax.ppermute(right, "tp", ring(n_tp, -1))
    return below, above, left, right


def gathered_early(x, n_tp):
    half = x.shape[1] // 2
    left, right = x[:, :half], x[:, half:]
    up, down = ring(n_tp, 1), ring(n_tp, -1)
    below_left = lax.ppermute(left, "tp", up)
    above_right = lax.ppermute(right, "tp", down)
    below_right = lax.ppermute(right, "tp", up)
    above_left = lax.ppermute(left, "tp", down)
    away_left = lax.ppermute(below_left, "tp", up)
    away_right = lax.ppermute(above_right, "tp", down)
    return (x, above_left, above_right, away_left, away_right, below_left, below_right)


def summed_over_tp(up1, dn1, up2, dn2, mine, n_tp):
    half = up2.shape[1]
    from_below = lax.ppermute(up1, "tp", ring(n_tp, 1))
    from_above = lax.ppermute(dn1, "tp", ring(n_tp, -1))
    add = lambda a, b: (a.astype(F32) + b.astype(F32)).astype(BF)
    up2 = add(up2, from_below[:, :half])
    dn2 = add(dn2, from_above[:, :half])
    left = lax.ppermute(up2, "tp", ring(n_tp, 1))
    right = lax.ppermute(dn2, "tp", ring(n_tp, -1))
    far = jnp.concatenate([left, right], axis=1).astype(F32)
    near = jnp.concatenate([from_above[:, half:], from_below[:, half:]], axis=1).astype(F32)
    return (mine.astype(F32) + far + near).astype(BF)


def combine_kernel(col_ref, cot_ref, back_ref, out_ref):
    tokens, top = col_ref.shape
    at = iota((tokens, back_ref.shape[0]), 1)
    hit = col_ref[:, 0:1] == at
    for k in range(1, top):
        hit = hit | (col_ref[:, k : k + 1] == at)
    total = jnp.dot(hit.astype(F32).astype(BF), back_ref[...], preferred_element_type=F32)
    out_ref[...] = (cot_ref[...].astype(F32) + total).astype(BF)


def combine(col, cot_part, back):
    return pl.pallas_call(
        combine_kernel,
        out_shape=jax.ShapeDtypeStruct(cot_part.shape, BF),
        compiler_params=params(16),
        name="combine",
    )(col, cot_part, back)


def pieces_of(rank_ref, z_refs, n_tp):
    z0, z_below, z_above, z_top, z_bottom = z_refs
    me = rank_ref[0]
    away = jnp.concatenate([z_top[...], z_bottom[...]], axis=1)
    order = ((0, z0[...]), (n_tp - 1, z_below[...]), (1, z_above[...]), (2, away))
    width = z0.shape[1]
    return [(pl.multiple_of(lax.rem(me + a, n_tp) * width, width), z) for a, z in order]


def state_kernel(rank_ref, z0, z1, z2, z3, z4, *refs, n_tp):
    sources, (branch_grad_ref, state_ref, carry_ref) = refs[:6], refs[6:9]
    holds, sems = refs[9:15], refs[15]
    copies = [pltpu.make_async_copy(a, b, sems.at[i]) for i, (a, b) in enumerate(zip(sources, holds))]
    for copy in copies:
        copy.start()
    copies[0].wait()
    w_ref, mixed_ref, branch_ref, decay_ref, later_ref, earlier_ref = holds
    total = None
    for at, z in pieces_of(rank_ref, (z0, z1, z2, z3, z4), n_tp):
        term = jnp.dot(z, w_ref[pl.ds(at, z.shape[1]), :], preferred_element_type=F32)
        total = term if total is None else total + term
    for copy in copies[1:]:
        copy.wait()
    branch_grad_ref[...] = (total * mixed_ref[...].astype(F32)).astype(BF)
    state = total * branch_ref[...].astype(F32)
    state_ref[...] = state
    scaled = state * decay_ref[...]
    ahead = jnp.sum(scaled * earlier_ref[...], axis=0, keepdims=True)
    behind = jnp.sum(scaled * later_ref[...], axis=0, keepdims=True)
    last = slice(state.shape[0] - 1, state.shape[0])
    through = decay_ref[last, :] * earlier_ref[last, :]
    lanes = carry_ref.shape[2]
    count = ahead.shape[1] // lanes
    tile = jnp.concatenate(
        [
            v[:, b * lanes : (b + 1) * lanes]
            for v in (ahead, behind, through, through)
            for b in range(count)
        ],
        axis=0,
    )
    carry_ref[...] = jnp.broadcast_to(tile[None], carry_ref.shape)


def state_grads(rank, zs, w_out, mixed, branch, decay, later_prod, earlier_prod, n_sp, n_tp):
    tokens, channels = mixed.shape
    full = lambda *shape: pl.BlockSpec(shape, lambda i: (0,) * len(shape))
    held = full(tokens, channels)
    carry = (n_sp, 16, channels // 4)
    sources = (w_out, mixed, branch, decay, later_prod, earlier_prod)
    return pl.pallas_call(
        functools.partial(state_kernel, n_tp=n_tp),
        grid=(1,),
        in_specs=[pl.BlockSpec(memory_space=pltpu.SMEM)]
        + [full(*z.shape) for z in zs]
        + [pl.BlockSpec(memory_space=pl.ANY)] * len(sources),
        out_specs=(held, held, full(*carry)),
        out_shape=(hbm((tokens, channels)), hbm((tokens, channels), F32), hbm(carry, F32)),
        scratch_shapes=[pltpu.VMEM(a.shape, a.dtype) for a in sources]
        + [pltpu.SemaphoreType.DMA((len(sources),))],
        compiler_params=params(32),
        name="state_grads",
    )(rank, *zs, *in_hbm(*sources))


def proj_kernel(rank_ref, core_ref, z_ref, own, above, left, right, below, keep_ref, send_ref, *, n_tp, size):
    z = z_ref[...]
    me = rank_ref[0]
    same = lax.rem(me + core_ref[0], 2) == 0

    def term(ahead):
        if ahead == 2:
            channels = jnp.concatenate([left[...], right[...]], axis=1)
        else:
            channels = {0: own, 1: above, 3: below}[ahead][...]
        return lax.dot_general(z, channels, COLS_COLS, preferred_element_type=F32).astype(BF)

    for a, b in ((0, 1), (2, 3)):
        first, second = term(a), term(b)
        at = [lax.rem(me + ahead, n_tp) // 2 for ahead in (a, b)]
        kept = jnp.where(same, at[0], at[1]) * size
        sent = jnp.where(same, at[1], at[0]) * size
        for i in range(first.shape[0] // size):
            rows = slice(i * size, (i + 1) * size)
            base = i * (n_tp // 2) * size
            keep_ref[pl.ds(pl.multiple_of(base + kept, size), size), :] = jnp.where(
                same, first[rows], second[rows]
            )
            send_ref[pl.ds(pl.multiple_of(base + sent, size), size), :] = jnp.where(
                same, second[rows], first[rows]
            )


def proj_terms(rank, core, z, gateds, n_tp, n_sp):
    features, channels = z.shape[1], gateds[0].shape[1]
    size = features * n_tp // n_sp
    half = jax.ShapeDtypeStruct((features * n_tp // 2, channels), BF)
    return pl.pallas_call(
        functools.partial(proj_kernel, n_tp=n_tp, size=size),
        in_specs=[pl.BlockSpec(memory_space=pltpu.SMEM)] * 2
        + [pl.BlockSpec(memory_space=pltpu.VMEM)] * 6,
        out_shape=(half, half),
        compiler_params=params(20),
        name="proj_terms",
    )(rank, core, z, *gateds)


def carried_in(me, got_ref):
    count, half = got_ref.shape[0], got_ref.shape[1] // 2
    carry = lambda q: got_ref[q, :half, :]
    through = lambda q: got_ref[q, half:, :]
    zero = jnp.zeros((half, got_ref.shape[2]), F32)
    ahead, behind = zero, zero
    for q in range(count):
        p = count - 1 - q
        ahead = jnp.where(p > me, carry(p) + through(p) * ahead, ahead)
        behind = jnp.where(q < me, carry(q) + through(q) * behind, behind)
    return ahead[: half // 2], behind[half // 2 :]


def final_kernel(me_ref, *refs):
    sources, out_ref = refs[:9], refs[9]
    later_ref, earlier_ref = refs[10:12]
    holds, sems = refs[12:21], refs[21]
    copies = [pltpu.make_async_copy(a, b, sems.at[i]) for i, (a, b) in enumerate(zip(sources, holds))]
    for copy in copies:
        copy.start()
    for copy in copies[:3]:
        copy.wait()
    got_ref, state_ref, decay_ref, h_later, h_earlier, q_ref, r_ref, rec_w, inp_w = holds
    rows = state_ref.shape[0]
    ahead, behind = carried_in(me_ref[0], got_ref)
    spread = lambda v: jnp.concatenate([v[b : b + 1] for b in range(v.shape[0])], axis=1)

    def step(i, carry):
        ahead, behind = carry
        t = rows - 1 - i
        later = state_ref[pl.ds(t, 1), :] + ahead
        later_ref[pl.ds(t, 1), :] = later
        earlier = state_ref[pl.ds(i, 1), :] + behind
        earlier_ref[pl.ds(i, 1), :] = earlier
        return (later * decay_ref[pl.ds(t, 1), :], earlier * decay_ref[pl.ds(i, 1), :])

    lax.fori_loop(0, rows, step, (spread(ahead), spread(behind)), unroll=8)
    for copy in copies[3:]:
        copy.wait()
    later, earlier = later_ref[...], earlier_ref[...]
    total = later + earlier
    h_later, h_earlier = h_later[...].astype(F32), h_earlier[...].astype(F32)
    rec_pre = (later * h_later + earlier * h_earlier).astype(BF)
    inp_pre = (total * q_ref[...].astype(F32)).astype(BF)
    direct = total * r_ref[...].astype(F32)
    size = rec_w.shape[1]
    for b in range(rec_w.shape[0]):
        cols = slice(b * size, (b + 1) * size)
        term = lax.dot_general(rec_pre[:, cols], rec_w[b], ROWS_ROWS, preferred_element_type=F32)
        term = term + lax.dot_general(
            inp_pre[:, cols], inp_w[b], ROWS_ROWS, preferred_element_type=F32
        )
        out_ref[:, cols] = (direct[:, cols] + term).astype(BF)


def final_grads(me, got, arrays, rec_w, inp_w):
    tokens, channels = arrays[0].shape
    sources = (got, *arrays, rec_w, inp_w)
    return pl.pallas_call(
        final_kernel,
        grid=(1,),
        in_specs=[pl.BlockSpec(memory_space=pltpu.SMEM)]
        + [pl.BlockSpec(memory_space=pl.ANY)] * len(sources),
        out_specs=pl.BlockSpec((tokens, channels), lambda i: (0, 0)),
        out_shape=hbm((tokens, channels)),
        scratch_shapes=[pltpu.VMEM((tokens, channels), F32)] * 2
        + [pltpu.VMEM(a.shape, a.dtype) for a in sources]
        + [pltpu.SemaphoreType.DMA((len(sources),))],
        compiler_params=params(24),
        name="final_grads",
    )(me, *in_hbm(*sources))


def blockwise(rows, weights):
    size = weights.shape[1]
    return jnp.concatenate(
        [
            jnp.dot(rows[:, b * size : (b + 1) * size], weights[b], preferred_element_type=F32)
            for b in range(weights.shape[0])
        ],
        axis=1,
    )


def shards(
    output_cotangent,
    chosen_expert_index,
    chosen_expert_weight,
    expert_slot_tokens,
    expert_gate_matrix,
    expert_up_matrix,
    expert_down_matrix,
    output_projection_matrix,
    recurrence_input,
    branch_activation_values,
    forward_scan_state,
    reverse_scan_state,
    channel_decay_rate,
    position_extra_log_decay,
    recurrence_gate_weights,
    input_gate_weights,
):
    n_sp = lax.axis_size("sp")
    n_tp = lax.axis_size("tp")
    tokens, model_width = output_cotangent.shape
    experts = n_sp * expert_gate_matrix.shape[0]
    capacity = expert_slot_tokens.shape[1] // n_sp
    slots = expert_slot_tokens.shape[1]
    hidden = expert_gate_matrix.shape[2]
    part = model_width // n_tp
    rank = lax.axis_index("tp").astype(jnp.int32).reshape(1)
    place = lax.axis_index("sp").astype(jnp.int32).reshape(1)
    bounds, at = [], 0
    for size in SLOT_GROUPS:
        bounds.append((at, size))
        at += size

    chosen_t, weight_t = chosen_expert_index.T, chosen_expert_weight.T
    w_gate, w_up, w_down = expert_gate_matrix[0], expert_up_matrix[0], expert_down_matrix[0]
    received = []
    for g, (base, size) in enumerate(bounds):
        width = model_width if g else part
        column = jnp.zeros_like(rank) if g else rank
        out = dispatch(
            column,
            chosen_t,
            weight_t,
            output_cotangent if g else in_hbm(output_cotangent)[0],
            width,
            base * experts,
            size * experts,
            experts,
        )
        got = lax.all_to_all(out.reshape(experts, size, -1), "sp", 0, 0, tiled=True)
        got = got.reshape(n_sp * size, -1)
        if g:
            received.append((got,))
        else:
            received.append(gathered_early(got, n_tp))
    down_turned, w_cat = fetched_weights(rank, w_down, w_gate, w_up, n_tp)

    by_source = expert_slot_tokens.reshape(n_sp, capacity, model_width)
    saved, acts, slopes = [], [], []
    for g, (base, size) in enumerate(bounds):
        x = by_source[:, base : base + size].reshape(n_sp * size, model_width)
        act, slope = expert_forward(x, (w_cat,) if g else (w_gate, w_up), hidden)
        saved.append(x)
        acts.append(act)
        slopes.append(slope)

    rec = jax.nn.sigmoid(blockwise(recurrence_input, recurrence_gate_weights))
    inp = jax.nn.sigmoid(blockwise(recurrence_input, input_gate_weights))
    rate = -gate_scale_factor * channel_decay_rate[None, :]
    log_decay = rec * rate + position_extra_log_decay[:, None]
    decay = jnp.exp(log_decay)
    scale_in = jnp.sqrt(-jnp.expm1(2.0 * log_decay))
    inputs = recurrence_input.astype(F32)
    xin = scale_in * inp * inputs
    mixed = (
        (decay * forward_scan_state + xin) + (decay * reverse_scan_state + xin)
    ).astype(BF)
    gated = (mixed.astype(F32) * branch_activation_values.astype(F32)).astype(BF)
    lower = (iota((tokens, tokens), 1) <= iota((tokens, tokens), 0)).astype(F32)
    running = jnp.dot(lower, log_decay, precision=lax.Precision.HIGHEST)
    later_prod = jnp.exp(running[-1:] - running)
    earlier_prod = jnp.exp(running - log_decay)
    rec_slope = rate * rec * (1.0 - rec)
    shared = inp * inputs * decay * decay / scale_in
    h_later = ((forward_scan_state * decay - shared) * rec_slope).astype(BF)
    h_earlier = ((reverse_scan_state * decay - shared) * rec_slope).astype(BF)
    q = (scale_in * inputs * inp * (1.0 - inp)).astype(BF)
    r = (scale_in * inp).astype(BF)

    boths, sums = [], []
    for g, (base, size) in enumerate(bounds):
        weights = (w_down, w_gate, w_up) if g else (down_turned, w_cat)
        both, *terms = expert_backward(rank, received[g], slopes[g], weights, n_tp)
        sums.append(summed_over_tp(*terms, n_tp).reshape(n_sp, size, part))
        boths.append(both)
    back = lax.all_to_all(jnp.concatenate(sums, axis=1), "sp", 0, 0, tiled=True)
    gate_grad, up_grad = gate_up_grads(saved, boths)
    down_grad = down_grads(rank, acts, received, n_tp)

    below, above, left, right = gathered_over_tp(gated, n_tp)
    gateds = (gated, above, left, right, below)

    cot_part = lax.dynamic_slice_in_dim(output_cotangent, rank[0] * part, part, 1)
    col = slot_columns(chosen_expert_index, experts)
    z0 = combine(col, cot_part, back.reshape(slots, part))
    zs = (z0, *gathered_over_tp(z0, n_tp))

    keep, send = proj_terms(rank, place % 2, z0, gateds, n_tp, n_sp)
    other = lax.ppermute(send, "sp", [(i, i ^ 1) for i in range(n_sp)])
    terms = (keep.astype(F32) + other.astype(F32)).astype(BF)
    terms = terms.reshape(n_sp // 2, model_width // n_sp, -1)
    groups = [list(range(c, n_sp, 2)) for c in range(2)]
    terms = lax.all_to_all(terms, "sp", 0, 0, axis_index_groups=groups, tiled=True)
    proj_grad = jnp.sum(terms.astype(F32), axis=0)
    spread = n_sp // n_tp
    moves = [
        (s * n_tp + x, (x * spread + s // n_tp) * n_tp + s % n_tp)
        for s in range(n_sp)
        for x in range(n_tp)
    ]
    proj_grad = lax.ppermute(proj_grad, ("sp", "tp"), moves)

    branch_grad, state, carry = state_grads(
        rank,
        zs,
        output_projection_matrix,
        mixed,
        branch_activation_values,
        decay,
        later_prod,
        earlier_prod,
        n_sp,
        n_tp,
    )
    carried = lax.all_to_all(carry, "sp", 0, 0, tiled=True)
    input_grad = final_grads(
        place,
        carried,
        (state, decay, h_later, h_earlier, q, r),
        recurrence_gate_weights,
        input_gate_weights,
    )
    return (gate_grad[None], up_grad[None], down_grad[None], proj_grad, branch_grad, input_grad)


def solution(mesh):
    in_specs = (
        P("sp", None),
        P("sp", None),
        P("sp", None),
        P("sp", None, None),
        P("sp", None, "tp"),
        P("sp", None, "tp"),
        P("sp", "tp", None),
        P(None, "tp"),
        P("sp", "tp"),
        P("sp", "tp"),
        P("sp", "tp"),
        P("sp", "tp"),
        P("tp"),
        P("sp"),
        P("tp", None, None),
        P("tp", None, None),
    )
    out_specs = (
        P("sp", None, "tp"),
        P("sp", None, "tp"),
        P("sp", "tp", None),
        P("sp", "tp"),
        P("sp", "tp"),
        P("sp", "tp"),
    )
    return jax.shard_map(shards, mesh=mesh, in_specs=in_specs, out_specs=out_specs, check_vma=False)
```
